256 devices in a mesh: grp: 2 (over z), tp: 16 (over y, core), dp: 8 (over x).
Axes of the slice: x: 8, y: 8, z: 2, core: 2. Of those that a mesh axis runs over, the one named last changes fastest.
The devices are a block of a 8x8x16 slice.
Arguments:
- tokens: bfloat16 [512, 2048], P(('grp', 'tp'), 'dp'), parts along dimension 0, may hold values from -25 to 25
- state: float32 [2, 512, 16, 128, 128], P(None, ('grp', 'dp'), 'tp'), parts along dimension 1, may hold values from -1 to 1
- lengths: int32 [512], P(('grp', 'dp')), parts along dimension 0, may hold values from 1 to 4096, 131072 in all
- norm_gain: bfloat16 [2, 2048], P(None, 'dp'), may hold values from 0.099609375 to 1.8984375
- w_query: bfloat16 [2, 2048, 2048], P(None, 'dp', 'tp'), may hold values from -0.125 to 0.125
- w_forget: bfloat16 [2, 2048, 2048], P(None, 'dp', 'tp'), may hold values from -0.125 to 0.125
- w_input: bfloat16 [2, 2048, 2048], P(None, 'dp', 'tp'), may hold values from -0.125 to 0.125
- w_gate: bfloat16 [2, 2048, 2048], P(None, 'dp', 'tp'), may hold values from -0.125 to 0.125
- w_out: bfloat16 [2, 2048, 2048], P(None, 'tp', 'dp'), may hold values from -0.125 to 0.125
- bound_logit: float32 [2, 2048], P(None, 'tp'), may hold values from -3 to 5
- pace: float32 [2, 2048], P(None, 'tp'), may hold values from 0.6 to 2
- head_gain: float32 [2, 128], replicated, may hold values from 0.4 to 2.5
Outputs:
- mixed: float32 [512, 2048], P(('grp', 'tp'), 'dp'), parts along dimension 0
- new_state: float32 [2, 512, 16, 128, 128], P(None, ('grp', 'dp'), 'tp'), parts along dimension 1
The draws below stay inside these ranges and needn't reach their ends.
There are 2 independent parts, one for each index of `grp`. The reference program is written for one: setup_inputs(seed, part) draws one part's arguments, and reference() takes and returns one part's arrays. A program takes and returns all parts, laid end to end along the dimension named above; an argument that names none is the same for every part. Nothing has to cross between parts.
All inputs are finite; a program needn't handle non-finite values. No bound on the sum of `lengths` on one device may be relied on, other than what follows from the above.
Results may differ from the reference program's by a relative error of at most 0.0083.
Values may be sent and summed in bfloat16 or wider, within the bound.
No kernel may reach another device: no remote copies, remote signals or barrier semaphores. Data moves between devices by JAX's collectives and lax.ppermute only.
A program may use at most 64 MiB of HBM per device.

```python
import math
import jax
import jax.numpy as jnp
import numpy as np
from jax import lax

D = 2048
HEADS = 16
HEAD = 128
KW = 2048
BATCH = 256
LENGTH_MEAN = 512
LONGEST = 4096


def draw_tokens(key, part):
    first, second = jax.random.split(jax.random.fold_in(key, 11), 2)
    level = jnp.exp(jax.random.uniform(second, (16,), jnp.float32, -1.2, 0.0))
    level = jnp.repeat(level, D // 16)
    base = jax.random.normal(first, (BATCH, D), jnp.float32)
    return jnp.clip(base * level[None, :], -25.0, 25.0).astype(jnp.bfloat16)


def draw_bound_logit(key, part):
    first, second, third = jax.random.split(jax.random.fold_in(key, 23), 3)
    quick = jax.random.bernoulli(first, 0.5, (2, HEADS))
    quick = jnp.repeat(quick, HEAD, axis=1)
    fast_values = jax.random.uniform(second, (2, KW), jnp.float32, -3.0, -1.0)
    slow_values = jax.random.uniform(third, (2, KW), jnp.float32, 2.0, 5.0)
    return jnp.where(quick, fast_values, slow_values).astype(jnp.float32)


def levels(stream_key, dims, shards, low, top_value):
    factor_of = 1.0
    for dim, blocks in shards:
        heights = jax.random.uniform(jax.random.fold_in(jax.random.fold_in(stream_key, 6), dim), (blocks,), jnp.float32, low / len(shards), top_value / len(shards))
        factor_of = factor_of * jnp.repeat(jnp.exp(heights), dims[dim] // blocks).reshape((-1,) + (1,) * (len(dims) - 1 - dim))
    return factor_of


def length_profile(amount, total, bound, lean):
    weights = [(1 << 20) // math.isqrt(standing ** lean) + 1 for standing in range(2, amount + 1)]
    rest, holding = total - bound - (amount - 1), [1] * (amount - 1)
    while rest > 0:
        candidates = [i for i in range(amount - 1) if holding[i] < bound]
        pool, remaining = sum([weights[i] for i in candidates]), rest
        for i in candidates:
            more = min(bound - holding[i], max(1, remaining * weights[i] // pool), rest)
            holding[i] = holding[i] + more
            rest = rest - more
    return np.array([bound] + holding)


def ragged_sizes(rng, amount, total, bound, skew):
    if amount == 2:
        one = jax.random.randint(rng, (), max(1, total - bound), min(bound, total - 1) + 1)
        return jnp.stack([one, total - one])
    sizes = jnp.asarray(length_profile(amount, total, bound, skew), jnp.int32)
    pairs = (amount - 1) // 2
    giver, taker = sizes[1:1 + 2 * pairs:2], sizes[2:2 + 2 * pairs:2]
    slack = jnp.minimum(giver - 1, bound - taker)
    shifted = jax.random.randint(jax.random.fold_in(rng, 1), (pairs,), 0, 1 << 20) % (slack + 1)
    sizes = sizes.at[1:1 + 2 * pairs:2].set(giver - shifted).at[2:2 + 2 * pairs:2].set(taker + shifted)
    return sizes[jax.random.permutation(jax.random.fold_in(rng, 2), amount)]


def noise(own_key, shape, deviation, most, cuts=(), kind=jnp.bfloat16):
    loudness = levels(own_key, shape, cuts, -0.22, 0.18) if cuts else 1.0
    entries = jax.random.normal(own_key, shape, jnp.float32) * deviation * loudness
    return jnp.minimum(jnp.maximum(entries, -most), most).astype(kind)


def setup_inputs(seed: int = 0, part: int = 0) -> dict:
    streams_of = jax.random.split(jax.random.key(seed), 13)
    own_keys = jax.random.split(jax.random.fold_in(streams_of[12], part), 13)
    tokens = draw_tokens(jax.random.fold_in(jax.random.fold_in(streams_of[12], part), 71), part)
    state = noise(own_keys[1], (2, BATCH, HEADS, HEAD, HEAD), 0.15, 1.0, ((1, 8), (2, 16)), jnp.float32)
    lengths = ragged_sizes(own_keys[2], BATCH, BATCH * LENGTH_MEAN, LONGEST, 2).astype(jnp.int32)
    norm_gain = jnp.clip(1.0 + 0.18 * jax.random.normal(streams_of[3], (2, D), jnp.float32), 0.099609375, 1.8984375).astype(jnp.bfloat16)
    w_query = noise(streams_of[4], (2, D, KW), D ** -0.5, 0.125, ((1, 8), (2, 16)))
    w_forget = noise(streams_of[5], (2, D, KW), D ** -0.5, 0.125, ((1, 8), (2, 16)))
    w_input = noise(streams_of[6], (2, D, KW), D ** -0.5, 0.125, ((1, 8), (2, 16)))
    w_gate = noise(streams_of[7], (2, D, KW), D ** -0.5, 0.125, ((1, 8), (2, 16)))
    w_out = noise(streams_of[8], (2, KW, D), KW ** -0.5, 0.125, ((1, 16), (2, 8)))
    bound_logit = draw_bound_logit(jax.random.fold_in(streams_of[12], 71), part)
    pace = jnp.clip(jnp.exp(math.log(2.0) - 1.2039728 * jax.random.uniform(streams_of[10], (2, KW), jnp.float32) ** levels(streams_of[10], (2, KW), ((1, 16),), -0.2, 0.2)), 0.6, 2.0)
    head_gain = jnp.clip(jnp.exp(jax.random.uniform(streams_of[11], (2, HEAD), jnp.float32, math.log(0.4), math.log(2.5))), 0.4, 2.5)
    return {"tokens": tokens, "state": state, "lengths": lengths, "norm_gain": norm_gain, "w_query": w_query, "w_forget": w_forget, "w_input": w_input, "w_gate": w_gate, "w_out": w_out, "bound_logit": bound_logit, "pace": pace, "head_gain": head_gain}


epsilon = 1e-06

def advance(prior, query, forget_in, value, gate, lower, pace_row, log_len, gain_row):
    count, width = query.shape
    size = prior.shape[-1]
    heads = width // size
    pre = forget_in - pace_row[None, :] * log_len[:, None]
    forget = lower[None, :] + (1.0 - lower[None, :]) * jax.nn.sigmoid(pre)
    key = (1.0 - lower[None, :]) * jax.nn.sigmoid(-pre)
    forget = forget.reshape(count, heads, size)
    key = key.reshape(count, heads, size)
    values = value.reshape(count, heads, size)
    updated = forget[..., None] * prior + key[..., None] * values[:, :, None, :]
    readout = jnp.einsum('bhk,bhkv->bhv', query.reshape(count, heads, size), updated, precision=lax.Precision.HIGHEST)
    normed = readout * lax.rsqrt(lax.optimization_barrier(jnp.mean(readout * readout, axis=-1, keepdims=True)) + epsilon)
    gates = gate.reshape(count, heads, size)
    normed = normed * gain_row[None, None, :] * jax.nn.silu(gates)
    return (updated, normed.reshape(count, width).astype(jnp.bfloat16))

def reference(tokens, state, lengths, norm_gain, w_query, w_forget, w_input, w_gate, w_out, bound_logit, pace, head_gain):
    current = tokens
    log_len = jnp.log(lengths.astype(jnp.float32) / LENGTH_MEAN)
    states = []
    result = None
    for block in range(2):
        wide = current.astype(jnp.float32)
        squares = lax.optimization_barrier(jnp.sum(wide * wide, axis=1))
        scale = lax.rsqrt(squares / D + epsilon)
        gained = (wide * norm_gain[block].astype(jnp.float32)[None, :]).astype(jnp.bfloat16)
        made = []
        for weight in (w_query[block], w_forget[block], w_input[block], w_gate[block]):
            made.append(scale[:, None] * jnp.dot(gained, weight, preferred_element_type=jnp.float32))
        lower = jax.nn.sigmoid(bound_logit[block])
        updated, normed = advance(state[block], made[0], made[1], made[2], made[3], lower, pace[block], log_len, head_gain[block])
        states.append(updated)
        branch = jnp.dot(normed, w_out[block], preferred_element_type=jnp.float32)
        if block == 0:
            current = (wide + branch).astype(jnp.bfloat16)
        else:
            result = wide + branch
    return (result, jnp.stack(states))
```

```python
import functools

import jax
import jax.numpy as jnp
from jax import lax
from jax.experimental import pallas as pl
from jax.experimental.pallas import tpu as pltpu
from jax.sharding import PartitionSpec as P

D = 2048
LENGTH_MEAN = 512
EXTRA = 128
STEP = 8
FLOOR = 2.0**-80
PARAMS = pltpu.CompilerParams(vmem_limit_bytes=16 << 20)

epsilon = 1e-06


def exchange(x, axis):
    return lax.all_to_all(x, axis, split_axis=0, concat_axis=0, tiled=True)


def exchange_products(x, axis):
    return exchange(x.astype(jnp.float16), axis).astype(jnp.float32)


def exponent(squares):
    return jnp.ceil(0.5 * jnp.log2(jnp.maximum(squares, FLOOR)))


def lanes_of(columns, rows):
    lane = lax.broadcasted_iota(jnp.int32, (rows, EXTRA), 1)
    block = jnp.zeros((rows, EXTRA), jnp.float32)
    for n, column in enumerate(columns):
        block = jnp.where(lane == n, column, block)
    return block


def project_kernel(x_ref, gain_ref, wq_ref, wf_ref, wi_ref, wg_ref, out_ref):
    owners, rows, _ = out_ref.shape
    width = wq_ref.shape[-1]
    x = x_ref[...].reshape(owners * rows, x_ref.shape[-1]).astype(jnp.float32)
    squares = jnp.sum(x * x, axis=1, keepdims=True)
    power = exponent(squares)
    down = jnp.exp2(-power)
    factor = down * 2.0**13
    gained = (x * gain_ref[...].astype(jnp.float32)).astype(jnp.bfloat16)
    for n, w_ref in enumerate((wq_ref, wf_ref, wi_ref, wg_ref)):
        partial = jnp.dot(gained, w_ref[...], preferred_element_type=jnp.float32)
        out_ref[:, :, n * width : (n + 1) * width] = (factor * partial).reshape(owners, rows, width)
    mantissa = squares * down * down
    high = mantissa.astype(jnp.bfloat16).astype(jnp.float32)
    extra = lanes_of((power - 13.0, high, mantissa - high), owners * rows)
    out_ref[:, :, 4 * width :] = extra.reshape(owners, rows, EXTRA)


def project(whole, gain, weights, owners):
    rows = whole.shape[0] * whole.shape[1] // owners
    width = weights[0].shape[-1]
    return pl.pallas_call(
        project_kernel,
        out_shape=jax.ShapeDtypeStruct((owners, rows, 4 * width + EXTRA), jnp.float32),
        compiler_params=PARAMS,
        name="project",
    )(whole, gain, *weights)


def advance_kernel(block, parts_ref, shift_ref, bound_ref, gain_ref, prior_ref, *refs):
    new_ref, normed_ref, prior_s, new_s, in_sems, out_sems = refs[-6:]
    steps, _, _, size = prior_s.shape
    loads = [
        pltpu.make_async_copy(prior_ref.at[block, pl.ds(n * STEP, STEP), 0], prior_s.at[n], in_sems.at[n])
        for n in range(steps)
    ]
    stores = [
        pltpu.make_async_copy(new_s.at[n], new_ref.at[block, pl.ds(n * STEP, STEP), 0], out_sems.at[n])
        for n in range(steps)
    ]
    for load in loads:
        load.start()

    up = jnp.exp2(parts_ref[:, :, 4 * size : 4 * size + 1])
    mantissa = parts_ref[:, :, 4 * size + 1 : 4 * size + 2] + parts_ref[:, :, 4 * size + 2 : 4 * size + 3]
    whole = up * 2.0**13
    squares = jnp.sum(mantissa * whole * whole, axis=0)
    scale = lax.rsqrt(squares / D + epsilon)
    query, forget_in, value, gate = (
        scale * jnp.sum(parts_ref[:, :, n * size : (n + 1) * size] * up, axis=0) for n in range(4)
    )
    lower = jax.nn.sigmoid(bound_ref[...])
    pre = forget_in - shift_ref[...]
    forget = (lower + (1.0 - lower) * jax.nn.sigmoid(pre)).T
    key = ((1.0 - lower) * jax.nn.sigmoid(-pre)).T
    query = query.T
    gate = gain_ref[...] * (gate * jax.nn.sigmoid(gate))

    outs = []
    for n in range(steps):
        loads[n].wait()
        for m in range(STEP):
            at = slice(n * STEP + m, n * STEP + m + 1)
            updated = forget[:, at] * prior_s[n, m] + key[:, at] * value[at, :]
            new_s[n, m] = updated
            outs.append(jnp.sum(query[:, at] * updated, axis=0, keepdims=True))
        stores[n].start()
    readout = jnp.concatenate(outs, axis=0)
    mean = jnp.mean(readout * readout, axis=1, keepdims=True)
    normed = readout * lax.rsqrt(mean + epsilon) * gate
    normed_ref[...] = jnp.broadcast_to(normed.astype(jnp.bfloat16), normed_ref.shape)
    for store in stores:
        store.wait()


def advance(block, parts, shift, bound, gain_row, state, target):
    _, count, _, size, _ = state.shape
    owners = parts.shape[0]
    steps = count // STEP
    vmem, hbm = pl.BlockSpec(memory_space=pltpu.VMEM), pl.BlockSpec(memory_space=pltpu.HBM)
    extra = () if target is None else (target,)
    return pl.pallas_call(
        functools.partial(advance_kernel, block),
        in_specs=[vmem] * 4 + [hbm] * (1 + len(extra)),
        out_specs=[hbm, vmem],
        out_shape=[
            jax.ShapeDtypeStruct(state.shape, jnp.float32),
            jax.ShapeDtypeStruct((owners, count, size), jnp.bfloat16),
        ],
        scratch_shapes=[pltpu.VMEM((steps, STEP, size, size), jnp.float32)] * 2
        + [pltpu.SemaphoreType.DMA((steps,))] * 2,
        input_output_aliases={5: 0} if extra else {},
        compiler_params=PARAMS,
        name=f"advance{block}",
    )(parts, shift, bound, gain_row, state, *extra)


def branch_kernel(normed_ref, w_ref, out_ref):
    owners, rows, _ = out_ref.shape
    width = w_ref.shape[-1]
    normed = normed_ref[...].reshape(owners * rows, normed_ref.shape[-1])
    wide = normed.astype(jnp.float32)
    power = exponent(jnp.sum(wide * wide, axis=1, keepdims=True))
    total = jnp.dot(normed, w_ref[...], preferred_element_type=jnp.float32) * (jnp.exp2(-power) * 2.0**14)
    out_ref[:, :, :width] = total.reshape(owners, rows, width)
    out_ref[:, :, width:] = lanes_of((power - 14.0,), owners * rows).reshape(owners, rows, EXTRA)


def branch_parts(normed, weight, owners):
    rows = normed.shape[0] * normed.shape[1] // owners
    return pl.pallas_call(
        branch_kernel,
        out_shape=jax.ShapeDtypeStruct((owners, rows, weight.shape[1] + EXTRA), jnp.float32),
        compiler_params=PARAMS,
        name="branch",
    )(normed, weight)


def gathered(parts_ref):
    width = parts_ref.shape[-1] - EXTRA
    return jnp.sum(parts_ref[:, :, :width] * jnp.exp2(parts_ref[:, :, width : width + 1]), axis=0)


def next_kernel(parts_ref, x_ref, out_ref):
    x = (x_ref[...].astype(jnp.float32) + gathered(parts_ref)).astype(jnp.bfloat16)
    out_ref[...] = jnp.broadcast_to(x, out_ref.shape)


def final_kernel(parts_ref, x_ref, out_ref):
    out_ref[...] = x_ref[0].astype(jnp.float32) + gathered(parts_ref)


def shards(
    tokens,
    state,
    lengths,
    norm_gain,
    w_query,
    w_forget,
    w_input,
    w_gate,
    w_out,
    bound_logit,
    pace,
    head_gain,
):
    tp, dp = lax.axis_size("tp"), lax.axis_size("dp")
    log_len = jnp.log(lengths.astype(jnp.float32) / LENGTH_MEAN)
    copies = jnp.broadcast_to(tokens, (tp, *tokens.shape))
    target = None
    for block in range(2):
        whole = exchange(copies, "tp")
        weights = (w_query[block], w_forget[block], w_input[block], w_gate[block])
        parts = exchange_products(project(whole, norm_gain[block][None, :], weights, dp), "dp")
        shift = pace[block][None, :] * log_len[:, None]
        target, normed = advance(
            block, parts, shift, bound_logit[block][None, :], head_gain[block][None, :], state, target
        )
        parts = exchange_products(branch_parts(exchange(normed, "dp"), w_out[block], tp), "tp")
        if block == 0:
            copies = pl.pallas_call(
                next_kernel,
                out_shape=jax.ShapeDtypeStruct(copies.shape, jnp.bfloat16),
                compiler_params=PARAMS,
                name="next",
            )(parts, tokens)
        else:
            result = pl.pallas_call(
                final_kernel,
                out_shape=jax.ShapeDtypeStruct(tokens.shape, jnp.float32),
                compiler_params=PARAMS,
                name="final",
            )(parts, copies)
    return result, target


def solution(mesh):
    in_specs = (
        P(("grp", "tp"), "dp"),
        P(None, ("grp", "dp"), "tp", None, None),
        P(("grp", "dp")),
        P(None, "dp"),
        P(None, "dp", "tp"),
        P(None, "dp", "tp"),
        P(None, "dp", "tp"),
        P(None, "dp", "tp"),
        P(None, "tp", "dp"),
        P(None, "tp"),
        P(None, "tp"),
        P(),
    )
    out_specs = (P(("grp", "tp"), "dp"), P(None, ("grp", "dp"), "tp", None, None))
    return jax.shard_map(shards, mesh=mesh, in_specs=in_specs, out_specs=out_specs, check_vma=False)
```

```python
import functools

import jax
import jax.numpy as jnp
from jax import lax
from jax.experimental import pallas as pl
from jax.experimental.pallas import tpu as pltpu
from jax.sharding import PartitionSpec as P

D = 2048
LENGTH_MEAN = 512
FLOOR = 2.0**-80
EXTRA = 8
STEP = 8
PARAMS = pltpu.CompilerParams(vmem_limit_bytes=16 << 20)
WIDE_PARAMS = pltpu.CompilerParams(vmem_limit_bytes=51 << 20)
PREP_PARAMS = pltpu.CompilerParams(vmem_limit_bytes=54900 << 10)
VMEM = pl.BlockSpec(memory_space=pltpu.VMEM)
HBM = pl.BlockSpec(memory_space=pltpu.HBM)

epsilon = 1e-06


def exchange(x, axis):
    return lax.all_to_all(x, axis, split_axis=0, concat_axis=0, tiled=True)


def exchange_products(x, axis):
    return exchange(x.astype(jnp.float16), axis).astype(jnp.float32)


def prep_kernel(lengths_ref, pace_ref, gain_ref, bound_ref, head_ref, *refs):
    weights, shift_ref, rows, firsts, sems = refs[:4], refs[4], refs[5:8], refs[8:12], refs[12]
    copies = [pltpu.make_async_copy(w_ref.at[0], first, sems.at[n]) for n, (w_ref, first) in enumerate(zip(weights, firsts))]
    for copy in copies:
        copy.start()
    count = shift_ref.shape[1]
    log_len = jnp.log(lengths_ref[...].astype(jnp.float32) / LENGTH_MEAN)
    across = lax.broadcasted_iota(jnp.int32, (count, count), 0) == lax.broadcasted_iota(jnp.int32, (count, count), 1)
    column = jnp.sum(jnp.where(across, jnp.broadcast_to(log_len, (count, count)), 0.0), axis=1, keepdims=True)
    for block in range(shift_ref.shape[0]):
        shift_ref[block] = pace_ref[block : block + 1, :] * column
    for row, ref in zip(rows, (gain_ref, bound_ref, head_ref)):
        row[...] = ref[...].astype(jnp.float32)
    for copy in copies:
        copy.wait()


def prep(lengths, pace, rows, weights):
    blocks, size = pace.shape
    out = pl.pallas_call(
        prep_kernel,
        in_specs=[VMEM] * (2 + len(rows)) + [HBM] * len(weights),
        out_specs=[VMEM] * (1 + len(rows) + len(weights)),
        out_shape=[jax.ShapeDtypeStruct((blocks, *lengths.shape, size), jnp.float32)]
        + [jax.ShapeDtypeStruct(row.shape, jnp.float32) for row in rows]
        + [jax.ShapeDtypeStruct(w.shape[1:], w.dtype) for w in weights],
        scratch_shapes=[pltpu.SemaphoreType.DMA((len(weights),))],
        compiler_params=PREP_PARAMS,
        name="prep",
    )(lengths[None, :], pace, *rows, *weights)
    return out[0], out[1 : 1 + len(rows)], out[1 + len(rows) :]


def project_kernel(block, x_ref, gain_ref, wq_ref, wf_ref, wi_ref, wg_ref, out_ref):
    owners, size = out_ref.shape[0], out_ref.shape[-1]
    rows = (out_ref.shape[1] - EXTRA) // 4
    x = x_ref[...].reshape(owners * rows, x_ref.shape[-1]).astype(jnp.float32)
    squares = jnp.sum(x * x, axis=1, keepdims=True)
    power = jnp.ceil(0.5 * jnp.log2(jnp.maximum(squares, FLOOR)))
    down = jnp.exp2(-power)
    factor = down * 2.0**13
    gained = (x * gain_ref[block : block + 1, :]).astype(jnp.bfloat16)
    for n, w_ref in enumerate((wq_ref, wf_ref, wi_ref, wg_ref)):
        weight = w_ref[block] if len(w_ref.shape) == 3 else w_ref[...]
        partial = jnp.dot(gained, weight, preferred_element_type=jnp.float32)
        out_ref[:, n * rows : (n + 1) * rows, :] = (factor * partial).reshape(owners, rows, size)
    mantissa = squares * down * down
    high = mantissa.astype(jnp.bfloat16).astype(jnp.float32)
    lane = lax.broadcasted_iota(jnp.int32, (owners * rows, size), 1)
    table = jnp.where(lane == 0, power - 13.0, jnp.where(lane == 1, high, jnp.where(lane == 2, mantissa - high, 0.0)))
    table = table.T[:EXTRA, :]
    for owner in range(owners):
        window = owner * rows // size * size
        turned = table[:, window : window + size]
        if owner * rows > window:
            turned = pltpu.roll(turned, size - (owner * rows - window), 1)
        out_ref[owner, 4 * rows :, :] = turned


def project(block, whole, gain, weights, owners):
    rows = whole.shape[0] * whole.shape[1] // owners
    width = weights[0].shape[-1]
    return pl.pallas_call(
        functools.partial(project_kernel, block),
        out_shape=jax.ShapeDtypeStruct((owners, 4 * rows + EXTRA, width), jnp.float32),
        compiler_params=PARAMS,
        name="project",
    )(whole, gain, *weights)


def advance_kernel(block, parts_ref, shift_ref, bound_ref, gain_ref, prior_ref, *refs):
    new_ref, normed_ref, prior_s, new_s, in_sems, out_sems = refs[-6:]
    steps = prior_s.shape[0]
    owners, count, size = normed_ref.shape
    loads = [
        pltpu.make_async_copy(prior_ref.at[block, pl.ds(n * STEP, STEP), 0], prior_s.at[n], in_sems.at[n])
        for n in range(steps)
    ]
    stores = [
        pltpu.make_async_copy(new_s.at[n], new_ref.at[block, pl.ds(n * STEP, STEP), 0], out_sems.at[n])
        for n in range(steps)
    ]
    for load in loads:
        load.start()

    up = jnp.exp2(parts_ref[:, 4 * count, :].T[:count, :])
    mantissa = (parts_ref[:, 4 * count + 1, :] + parts_ref[:, 4 * count + 2, :]).T[:count, :]
    norms = up * 2.0**13
    squares = jnp.sum(mantissa * norms * norms, axis=1, keepdims=True)
    scale = lax.rsqrt(squares / D + epsilon)

    def whole(n):
        total = parts_ref[0, n * count : (n + 1) * count, :] * up[:, 0:1]
        for source in range(1, owners):
            total += parts_ref[source, n * count : (n + 1) * count, :] * up[:, source : source + 1]
        return scale * total

    query, forget_in, value, gate = (whole(n) for n in range(4))
    lower = jax.nn.sigmoid(bound_ref[block : block + 1, :])
    pre = forget_in - shift_ref[block]
    forget = (lower + (1.0 - lower) * jax.nn.sigmoid(pre)).T
    key = ((1.0 - lower) * jax.nn.sigmoid(-pre)).T
    query = query.T
    gate = gain_ref[block : block + 1, :] * (gate * jax.nn.sigmoid(gate))

    outs = []
    for n in range(steps):
        loads[n].wait()
        for m in range(STEP):
            at = slice(n * STEP + m, n * STEP + m + 1)
            updated = forget[:, at] * prior_s[n, m] + key[:, at] * value[at, :]
            new_s[n, m] = updated
            outs.append(jnp.sum(query[:, at] * updated, axis=0, keepdims=True))
        stores[n].start()
    readout = jnp.concatenate(outs, axis=0)
    mean = jnp.mean(readout * readout, axis=1, keepdims=True)
    normed = readout * lax.rsqrt(mean + epsilon) * gate
    normed_ref[...] = jnp.broadcast_to(normed.astype(jnp.bfloat16), normed_ref.shape)
    for store in stores:
        store.wait()


def advance(block, parts, shift, bound, gain_row, state, target):
    _, count, _, size, _ = state.shape
    steps = count // STEP
    extra = () if target is None else (target,)
    return pl.pallas_call(
        functools.partial(advance_kernel, block),
        in_specs=[VMEM] * 4 + [HBM] * (1 + len(extra)),
        out_specs=[HBM, VMEM],
        out_shape=[
            jax.ShapeDtypeStruct(state.shape, jnp.float32),
            jax.ShapeDtypeStruct((parts.shape[0], count, size), jnp.bfloat16),
        ],
        scratch_shapes=[pltpu.VMEM((steps, STEP, size, size), jnp.float32)] * 2
        + [pltpu.SemaphoreType.DMA((steps,))] * 2,
        input_output_aliases={5: 0} if extra else {},
        compiler_params=WIDE_PARAMS,
        name="advance",
    )(parts, shift, bound, gain_row, state, *extra)


def branch_kernel(block, normed_ref, w_ref, out_ref):
    normed = normed_ref[...].reshape(-1, normed_ref.shape[-1])
    total = jnp.dot(normed, w_ref[block], preferred_element_type=jnp.float32)
    root = jnp.sqrt(jnp.abs(total)) * 2.0**8
    out_ref[...] = jnp.where(total < 0.0, -root, root).reshape(out_ref.shape)


def branch_parts(block, normed, weight, owners):
    rows = normed.shape[0] * normed.shape[1] // owners
    return pl.pallas_call(
        functools.partial(branch_kernel, block),
        out_shape=jax.ShapeDtypeStruct((owners, rows, weight.shape[2]), jnp.float32),
        compiler_params=PARAMS,
        name="branch",
    )(normed, weight)


def gathered(parts_ref):
    parts = parts_ref[...]
    return jnp.sum(parts * jnp.abs(parts), axis=0) * 2.0**-16


def next_kernel(parts_ref, x_ref, out_ref):
    x = (x_ref[...].astype(jnp.float32) + gathered(parts_ref)).astype(jnp.bfloat16)
    out_ref[...] = jnp.broadcast_to(x, out_ref.shape)


def final_kernel(parts_ref, x_ref, out_ref):
    out_ref[...] = x_ref[0].astype(jnp.float32) + gathered(parts_ref)


def shards(
    tokens,
    state,
    lengths,
    norm_gain,
    w_query,
    w_forget,
    w_input,
    w_gate,
    w_out,
    bound_logit,
    pace,
    head_gain,
):
    tp, dp = lax.axis_size("tp"), lax.axis_size("dp")
    copies = jnp.broadcast_to(tokens, (tp, *tokens.shape))
    weights = (w_query, w_forget, w_input, w_gate)
    shift, (norm_gain, bound_logit, head_gain), firsts = prep(lengths, pace, (norm_gain, bound_logit, head_gain), weights)
    target = None
    for block in range(2):
        whole = exchange(copies, "tp")
        parts = exchange_products(project(block, whole, norm_gain, weights if block else firsts, dp), "dp")
        target, normed = advance(block, parts, shift, bound_logit, head_gain, state, target)
        parts = exchange_products(branch_parts(block, exchange(normed, "dp"), w_out, tp), "tp")
        if block == 0:
            copies = pl.pallas_call(
                next_kernel,
                out_shape=jax.ShapeDtypeStruct(copies.shape, jnp.bfloat16),
                compiler_params=PARAMS,
                name="next",
            )(parts, tokens)
        else:
            result = pl.pallas_call(
                final_kernel,
                out_shape=jax.ShapeDtypeStruct(tokens.shape, jnp.float32),
                compiler_params=PARAMS,
                name="final",
            )(parts, copies)
    return result, target


def solution(mesh):
    in_specs = (
        P(("grp", "tp"), "dp"),
        P(None, ("grp", "dp"), "tp", None, None),
        P(("grp", "dp")),
        P(None, "dp"),
        P(None, "dp", "tp"),
        P(None, "dp", "tp"),
        P(None, "dp", "tp"),
        P(None, "dp", "tp"),
        P(None, "tp", "dp"),
        P(None, "tp"),
        P(None, "tp"),
        P(),
    )
    out_specs = (P(("grp", "tp"), "dp"), P(None, ("grp", "dp"), "tp", None, None))
    return jax.shard_map(shards, mesh=mesh, in_specs=in_specs, out_specs=out_specs, check_vma=False)
```

```python
import functools

import jax
import jax.numpy as jnp
from jax import lax
from jax.experimental import pallas as pl
from jax.experimental.pallas import tpu as pltpu
from jax.sharding import PartitionSpec as P

D = 2048
LENGTH_MEAN = 512
FLOOR = 2.0**-80
PAD = 16
SHARE_AT = 16
STEP = 8
PARAMS = pltpu.CompilerParams(vmem_limit_bytes=16 << 20)
WIDE_PARAMS = pltpu.CompilerParams(vmem_limit_bytes=51 << 20)
SECOND_PARAMS = pltpu.CompilerParams(vmem_limit_bytes=49 << 20)
PACK_PARAMS = pltpu.CompilerParams(vmem_limit_bytes=54900 << 10)
VMEM = pl.BlockSpec(memory_space=pltpu.VMEM)
HBM = pl.BlockSpec(memory_space=pltpu.HBM)

epsilon = 1e-06


def exchange(x, axis):
    return lax.all_to_all(x, axis, split_axis=0, concat_axis=0, tiled=True)


def exchange_products(x, axis):
    return exchange(x.astype(jnp.float16), axis).astype(jnp.float32)


def pack_kernel(block, gain_ref, wq_ref, wf_ref, wi_ref, wg_ref, out_ref, sems):
    rows, size = wq_ref.shape[1:]
    copies = [
        pltpu.make_async_copy(w_ref.at[block], out_ref.at[pl.ds(0, rows), pl.ds(n * size, size)], sems.at[n])
        for n, w_ref in enumerate((wq_ref, wf_ref, wi_ref, wg_ref))
    ]
    for copy in copies:
        copy.start()
    gain = jnp.broadcast_to(gain_ref[block : block + 1, :].astype(jnp.float32), (PAD, rows))
    out_ref[rows:, :rows] = gain.astype(out_ref.dtype)
    out_ref[rows:, rows:] = jnp.zeros((PAD, 4 * size - rows), out_ref.dtype)
    for copy in copies:
        copy.wait()


def pack(block, gain, weights):
    _, rows, size = weights[0].shape
    return pl.pallas_call(
        functools.partial(pack_kernel, block),
        in_specs=[VMEM] + [HBM] * 4,
        out_specs=VMEM,
        out_shape=jax.ShapeDtypeStruct((rows + PAD, 4 * size), jnp.bfloat16),
        scratch_shapes=[pltpu.SemaphoreType.DMA((4,))],
        compiler_params=PACK_PARAMS,
        name="pack",
    )(gain, *weights)


def around(shard, axis):
    size = lax.axis_size(axis)
    onward = [(n, (n + 1) % size) for n in range(size)]
    back = [(n, (n - 1) % size) for n in range(size)]
    held = {0: shard}
    for step in range(1, size // 2 + 1):
        held[size - step] = lax.ppermute(held[(size - step + 1) % size], axis, onward)
        if step < size // 2:
            held[step] = lax.ppermute(held[step - 1], axis, back)
    return [held[n] for n in range(size)]


def selection(wide, narrow, first, share, transposed):
    shape = (narrow, wide) if transposed else (wide, narrow)
    long = lax.broadcasted_iota(jnp.int32, shape, 1 if transposed else 0)
    short = lax.broadcasted_iota(jnp.int32, shape, 0 if transposed else 1) - first
    inside = (short >= 0) & (short < share) & (long == lax.axis_index("tp") * share + short)
    return jnp.where(inside, 1.0, 0.0).astype(jnp.bfloat16)


def code(total):
    root = jnp.sqrt(jnp.abs(total)) * 2.0**6
    return jnp.where(total < 0.0, -root, root)


def project_kernel(share, x_ref, w_ref, out_ref):
    owners, size = out_ref.shape[0], out_ref.shape[-1]
    rows = out_ref.shape[1] // 5
    held = x_ref[...].reshape(owners * rows, x_ref.shape[-1])
    x = held.astype(jnp.float32)
    squares = jnp.sum(x * x, axis=1, keepdims=True)
    power = jnp.ceil(0.5 * jnp.log2(jnp.maximum(squares, FLOOR)))
    down = jnp.exp2(-power)
    factor = down * 2.0**13
    features = x.shape[1]
    gained = (x * w_ref[features : features + 1, :features].astype(jnp.float32)).astype(jnp.bfloat16)
    partial = factor * jnp.dot(gained, w_ref[:features, :], preferred_element_type=jnp.float32)
    for n in range(4):
        out_ref[:, n * rows : (n + 1) * rows, :] = partial[:, n * size : (n + 1) * size].reshape(owners, rows, size)
    mantissa = squares * down * down
    high = mantissa.astype(jnp.bfloat16).astype(jnp.float32)
    lane = lax.broadcasted_iota(jnp.int32, (owners * rows, size), 1)
    table = jnp.where(lane == 0, power - 13.0, jnp.where(lane == 1, high, jnp.where(lane == 2, mantissa - high, 0.0)))
    choose = selection(held.shape[1], size, SHARE_AT, share, False)
    kept = factor * jnp.dot(held, choose, preferred_element_type=jnp.float32)
    out_ref[:, 4 * rows :, :] = (table + kept).reshape(owners, rows, size)


def project(whole, weight, owners):
    rows = whole.shape[0] * whole.shape[1] // owners
    share = whole.shape[2] // lax.axis_size("tp")
    return pl.pallas_call(
        functools.partial(project_kernel, share),
        out_shape=jax.ShapeDtypeStruct((owners, 5 * rows, weight.shape[1] // 4), jnp.float32),
        compiler_params=PARAMS,
        name="project",
    )(whole, weight)


def moves(block, state_ref, new_ref, prior_s, new_s, in_sems, out_sems):
    steps = prior_s.shape[0]
    rows = [pl.ds(n * STEP, STEP) for n in range(steps)]
    loads = [pltpu.make_async_copy(state_ref.at[block, rows[n], 0], prior_s.at[n], in_sems.at[n]) for n in range(steps)]
    stores = [pltpu.make_async_copy(new_s.at[n], new_ref.at[block, rows[n], 0], out_sems.at[n]) for n in range(steps)]
    return loads, stores


def recur(block, made, shift_ref, bound_ref, head_ref, loads, stores, prior_s, new_s):
    query, forget_in, value, gate = made
    lower = jax.nn.sigmoid(bound_ref[block : block + 1, :])
    pre = forget_in - shift_ref[block]
    forget = (lower + (1.0 - lower) * jax.nn.sigmoid(pre)).T
    key = ((1.0 - lower) * jax.nn.sigmoid(-pre)).T
    query = query.T
    gate = head_ref[block : block + 1, :] * (gate * jax.nn.sigmoid(gate))
    outs = []
    for n in range(len(loads)):
        loads[n].wait()
        for m in range(STEP):
            at = slice(n * STEP + m, n * STEP + m + 1)
            updated = forget[:, at] * prior_s[n, m] + key[:, at] * value[at, :]
            new_s[n, m] = updated
            outs.append(jnp.sum(query[:, at] * updated, axis=0, keepdims=True))
        stores[n].start()
    readout = jnp.concatenate(outs, axis=0)
    mean = jnp.mean(readout * readout, axis=1, keepdims=True)
    return (readout * lax.rsqrt(mean + epsilon) * gate).astype(jnp.bfloat16)


def first_kernel(share, parts_ref, shift_ref, bound_ref, head_ref, *refs):
    shards, (state_ref, new_ref, out_ref, *scratch) = refs[:-7], refs[-7:]
    loads, stores = moves(0, state_ref, new_ref, *scratch)
    for load in loads:
        load.start()
    owners, _, size = parts_ref.shape
    count = out_ref.shape[1]
    made, squares = [0.0] * 4, 0.0
    for source in range(owners):
        table = parts_ref[source, 4 * count :, :]
        up = jnp.exp2(table[:, 0:1])
        norm = up * 2.0**13
        squares += (table[:, 1:2] + table[:, 2:3]) * norm * norm
        for n in range(4):
            made[n] += parts_ref[source, n * count : (n + 1) * count, :] * up
    scale = lax.rsqrt(squares / D + epsilon)
    made = [scale * total for total in made]
    normed = recur(0, made, shift_ref, bound_ref, head_ref, loads, stores, *scratch[:2])
    width = shards[0].shape[1]
    place = selection(width, size, SHARE_AT, share, True)
    for n, shard in enumerate(shards):
        chunk = lax.rem(lax.axis_index("dp") + n, owners)
        table = parts_ref[chunk, 4 * count :, :]
        branch = jnp.dot(normed, shard[...], preferred_element_type=jnp.float32)
        kept = jnp.dot(table.astype(jnp.bfloat16), place, preferred_element_type=jnp.float32)
        coded = code(branch + jnp.exp2(table[:, 0:1]) * kept)
        for part in range(width // size):
            out_ref[chunk * (width // size) + part] = coded[:, part * size : (part + 1) * size]
    for store in stores:
        store.wait()


def scratch_of(state):
    _, count, _, size, _ = state.shape
    steps = count // STEP
    return [pltpu.VMEM((steps, STEP, size, size), jnp.float32)] * 2 + [pltpu.SemaphoreType.DMA((steps,))] * 2


def first(parts, shift, bound, head, shards, state):
    _, count, _, size, _ = state.shape
    tp = lax.axis_size("tp")
    return pl.pallas_call(
        functools.partial(first_kernel, shards[0].shape[1] // tp),
        in_specs=[VMEM] * (4 + len(shards)) + [HBM],
        out_specs=[HBM, VMEM],
        out_shape=[
            jax.ShapeDtypeStruct(state.shape, jnp.float32),
            jax.ShapeDtypeStruct((tp, count, size), jnp.float32),
        ],
        scratch_shapes=scratch_of(state),
        compiler_params=WIDE_PARAMS,
        name="first",
    )(parts, shift, bound, head, *shards, state)


def decoded(parts_ref):
    parts = parts_ref[...]
    return jnp.sum(parts * jnp.abs(parts), axis=0) * 2.0**-12


def next_kernel(parts_ref, out_ref):
    out_ref[...] = jnp.broadcast_to(decoded(parts_ref).astype(jnp.bfloat16), out_ref.shape)


def second_kernel(share, x_ref, shift_ref, bound_ref, head_ref, *refs):
    shards, (state_ref, _, new_ref, out_ref, *scratch) = refs[:-8], refs[-8:]
    loads, stores = moves(1, state_ref, new_ref, *scratch)
    for load in loads:
        load.start()
    owners, _, size = out_ref.shape
    rows = shards[0].shape[0] - PAD
    parts = rows // size
    count = x_ref.shape[1]
    choose = selection(rows, size, 0, share, False)
    made, squares = 0.0, 0.0
    for n, shard in enumerate(shards):
        chunk = lax.rem(lax.axis_index("dp") + n, owners)
        held = jnp.concatenate([x_ref[chunk * parts + part] for part in range(parts)], axis=1)
        wide = held.astype(jnp.float32)
        squares += jnp.sum(wide * wide, axis=1, keepdims=True)
        gained = (wide * shard[rows : rows + 1, :rows].astype(jnp.float32)).astype(jnp.bfloat16)
        made += jnp.dot(gained, shard[:rows, :], preferred_element_type=jnp.float32)
        kept = jnp.dot(held, choose, preferred_element_type=jnp.float32)
        out_ref[chunk, count:, :] = kept.astype(jnp.bfloat16)
    made = lax.rsqrt(squares / D + epsilon) * made
    made = [made[:, n * size : (n + 1) * size] for n in range(4)]
    normed = recur(1, made, shift_ref, bound_ref, head_ref, loads, stores, *scratch[:2])
    out_ref[:, :count, :] = jnp.broadcast_to(normed, (owners, count, size))
    for store in stores:
        store.wait()


def second(x, shift, bound, head, shards, state, target):
    _, count, _, size, _ = state.shape
    rows = shards[0].shape[0] - PAD
    return pl.pallas_call(
        functools.partial(second_kernel, rows // lax.axis_size("tp")),
        in_specs=[VMEM] * (4 + len(shards)) + [HBM] * 2,
        out_specs=[HBM, VMEM],
        out_shape=[
            jax.ShapeDtypeStruct(state.shape, jnp.float32),
            jax.ShapeDtypeStruct((len(shards), 2 * count, size), jnp.bfloat16),
        ],
        scratch_shapes=scratch_of(state),
        input_output_aliases={5 + len(shards): 0},
        compiler_params=SECOND_PARAMS,
        name="second",
    )(x, shift, bound, head, *shards, state, target)


def branch_kernel(share, normed_ref, w_ref, out_ref):
    count, size = normed_ref.shape[1] // 2, normed_ref.shape[2]
    normed = normed_ref[:, :count, :].reshape(-1, size)
    held = normed_ref[:, count:, :].reshape(-1, size)
    weight = w_ref[1]
    total = jnp.dot(normed, weight, preferred_element_type=jnp.float32)
    place = selection(weight.shape[1], size, 0, share, True)
    total += jnp.dot(held, place, preferred_element_type=jnp.float32)
    out_ref[...] = code(total).reshape(out_ref.shape)


def branch_parts(normed, weight, owners):
    rows = normed.shape[0] * normed.shape[1] // 2 // owners
    return pl.pallas_call(
        functools.partial(branch_kernel, weight.shape[2] // owners),
        out_shape=jax.ShapeDtypeStruct((owners, rows, weight.shape[2]), jnp.float32),
        compiler_params=PARAMS,
        name="branch",
    )(normed, weight)


def final_kernel(parts_ref, out_ref):
    out_ref[...] = decoded(parts_ref)


def shards(
    tokens,
    state,
    lengths,
    norm_gain,
    w_query,
    w_forget,
    w_input,
    w_gate,
    w_out,
    bound_logit,
    pace,
    head_gain,
):
    tp, dp = lax.axis_size("tp"), lax.axis_size("dp")
    whole = exchange(jnp.broadcast_to(tokens, (tp, *tokens.shape)), "tp")
    weights = (w_query, w_forget, w_input, w_gate)
    back = around(w_out[0], "dp")
    weight = pack(0, norm_gain, weights)
    held = around(pack(1, norm_gain, weights), "dp")
    log_len = jnp.log(lengths.astype(jnp.float32) / LENGTH_MEAN)
    shift = pace[:, None, :] * log_len[None, :, None]

    parts = exchange_products(project(whole, weight, dp), "dp")
    target, parts = first(parts, shift, bound_logit, head_gain, back, state)
    parts = exchange_products(parts, "tp")
    copies = pl.pallas_call(
        next_kernel,
        out_shape=jax.ShapeDtypeStruct(parts.shape, jnp.bfloat16),
        compiler_params=PARAMS,
        name="next",
    )(parts)
    target, normed = second(exchange(copies, "tp"), shift, bound_logit, head_gain, held, state, target)
    parts = exchange_products(branch_parts(exchange(normed, "dp"), w_out, tp), "tp")
    result = pl.pallas_call(
        final_kernel,
        out_shape=jax.ShapeDtypeStruct(tokens.shape, jnp.float32),
        compiler_params=PARAMS,
        name="final",
    )(parts)
    return result, target


def solution(mesh):
    in_specs = (
        P(("grp", "tp"), "dp"),
        P(None, ("grp", "dp"), "tp", None, None),
        P(("grp", "dp")),
        P(None, "dp"),
        P(None, "dp", "tp"),
        P(None, "dp", "tp"),
        P(None, "dp", "tp"),
        P(None, "dp", "tp"),
        P(None, "tp", "dp"),
        P(None, "tp"),
        P(None, "tp"),
        P(),
    )
    out_specs = (P(("grp", "tp"), "dp"), P(None, ("grp", "dp"), "tp", None, None))
    return jax.shard_map(shards, mesh=mesh, in_specs=in_specs, out_specs=out_specs, check_vma=False)
```

```python
import functools

import jax
import jax.numpy as jnp
from jax import lax
from jax.experimental import pallas as pl
from jax.experimental.pallas import tpu as pltpu
from jax.sharding import PartitionSpec as P


D = 2048
LENGTH_MEAN = 512
FLOOR = 2.0**-80
PAD = 16
SHARE_AT = 16
STEP = 8
PARAMS = pltpu.CompilerParams(vmem_limit_bytes=16 << 20)
WIDE_PARAMS = pltpu.CompilerParams(vmem_limit_bytes=51 << 20)
SECOND_PARAMS = pltpu.CompilerParams(vmem_limit_bytes=49 << 20)
PREP_PARAMS = pltpu.CompilerParams(vmem_limit_bytes=54900 << 10)
PACK_PARAMS = pltpu.CompilerParams(vmem_limit_bytes=55300 << 10)
VMEM = pl.BlockSpec(memory_space=pltpu.VMEM)
HBM = pl.BlockSpec(memory_space=pltpu.HBM)

epsilon = 1e-06


def exchange(x, axis):
    return lax.all_to_all(x, axis, split_axis=0, concat_axis=0, tiled=True)


def exchange_products(x, axis):
    return exchange(x.astype(jnp.float16), axis).astype(jnp.float32)


def pack_kernel(block, gain_ref, wq_ref, wf_ref, wi_ref, wg_ref, out_ref, sems):
    rows, size = wq_ref.shape[1:]
    copies = [
        pltpu.make_async_copy(w_ref.at[block], out_ref.at[pl.ds(0, rows), pl.ds(n * size, size)], sems.at[n])
        for n, w_ref in enumerate((wq_ref, wf_ref, wi_ref, wg_ref))
    ]
    for copy in copies:
        copy.start()
    gain = jnp.broadcast_to(gain_ref[block : block + 1, :].astype(jnp.float32), (PAD, rows))
    out_ref[rows:, :rows] = gain.astype(out_ref.dtype)
    out_ref[rows:, rows:] = jnp.zeros((PAD, 4 * size - rows), out_ref.dtype)
    for copy in copies:
        copy.wait()


def pack(block, gain, weights):
    _, rows, size = weights[0].shape
    return pl.pallas_call(
        functools.partial(pack_kernel, block),
        in_specs=[VMEM] + [HBM] * 4,
        out_specs=VMEM,
        out_shape=jax.ShapeDtypeStruct((rows + PAD, 4 * size), jnp.bfloat16),
        scratch_shapes=[pltpu.SemaphoreType.DMA((4,))],
        compiler_params=PACK_PARAMS,
        name="pack",
    )(gain, *weights)


def prep_kernel(gain_ref, *refs):
    weights, row_ref, firsts, sems = refs[:4], refs[4], refs[5:9], refs[9]
    copies = [pltpu.make_async_copy(w_ref.at[0], out, sems.at[n]) for n, (w_ref, out) in enumerate(zip(weights, firsts))]
    for copy in copies:
        copy.start()
    row_ref[...] = gain_ref[0:1, :].astype(jnp.float32)
    for copy in copies:
        copy.wait()


def prep(gain, weights):
    return pl.pallas_call(
        prep_kernel,
        in_specs=[VMEM] + [HBM] * len(weights),
        out_specs=[VMEM] * (1 + len(weights)),
        out_shape=[jax.ShapeDtypeStruct((1, gain.shape[1]), jnp.float32)]
        + [jax.ShapeDtypeStruct(w.shape[1:], w.dtype) for w in weights],
        scratch_shapes=[pltpu.SemaphoreType.DMA((len(weights),))],
        compiler_params=PREP_PARAMS,
        name="prep",
    )(gain, *weights)


def after(x, y):
    return lax.optimization_barrier((x, y))[0]


def around(shard, axis, gates):
    size = lax.axis_size(axis)
    onward = [(n, (n + 1) % size) for n in range(size)]
    back = [(n, (n - 1) % size) for n in range(size)]
    held = {0: shard}
    for step in range(1, size // 2 + 1):
        left, right = held[size - step + 1 if step > 1 else 0], held[step - 1]
        if step in gates:
            left, right = after(left, gates[step]), after(right, gates[step])
        held[size - step] = lax.ppermute(left, axis, onward)
        if step < size // 2:
            held[step] = lax.ppermute(right, axis, back)
    return [held[n] for n in range(size)]


def selection(wide, narrow, first, share, transposed):
    shape = (narrow, wide) if transposed else (wide, narrow)
    long = lax.broadcasted_iota(jnp.int32, shape, 1 if transposed else 0)
    short = lax.broadcasted_iota(jnp.int32, shape, 0 if transposed else 1) - first
    inside = (short >= 0) & (short < share) & (long == lax.axis_index("tp") * share + short)
    return jnp.where(inside, 1.0, 0.0).astype(jnp.bfloat16)


def code(total):
    root = jnp.sqrt(jnp.abs(total)) * 2.0**6
    return jnp.where(total < 0.0, -root, root)


def project_kernel(share, x_ref, gain_ref, wq_ref, wf_ref, wi_ref, wg_ref, out_ref):
    owners, size = out_ref.shape[0], out_ref.shape[-1]
    rows = out_ref.shape[1] // 5
    held = x_ref[...].reshape(owners * rows, x_ref.shape[-1])
    x = held.astype(jnp.float32)
    squares = jnp.sum(x * x, axis=1, keepdims=True)
    power = jnp.ceil(0.5 * jnp.log2(jnp.maximum(squares, FLOOR)))
    down = jnp.exp2(-power)
    factor = down * 2.0**13
    gained = (x * gain_ref[...]).astype(jnp.bfloat16)
    for n, w_ref in enumerate((wq_ref, wf_ref, wi_ref, wg_ref)):
        partial = factor * jnp.dot(gained, w_ref[...], preferred_element_type=jnp.float32)
        out_ref[:, n * rows : (n + 1) * rows, :] = partial.reshape(owners, rows, size)
    mantissa = squares * down * down
    high = mantissa.astype(jnp.bfloat16).astype(jnp.float32)
    lane = lax.broadcasted_iota(jnp.int32, (owners * rows, size), 1)
    table = jnp.where(lane == 0, power - 13.0, jnp.where(lane == 1, high, jnp.where(lane == 2, mantissa - high, 0.0)))
    choose = selection(held.shape[1], size, SHARE_AT, share, False)
    kept = factor * jnp.dot(held, choose, preferred_element_type=jnp.float32)
    out_ref[:, 4 * rows :, :] = (table + kept).reshape(owners, rows, size)


def project(whole, gain, weights, owners):
    rows = whole.shape[0] * whole.shape[1] // owners
    share = whole.shape[2] // lax.axis_size("tp")
    return pl.pallas_call(
        functools.partial(project_kernel, share),
        out_shape=jax.ShapeDtypeStruct((owners, 5 * rows, weights[0].shape[1]), jnp.float32),
        compiler_params=PARAMS,
        name="project",
    )(whole, gain, *weights)


def moves(block, state_ref, new_ref, prior_s, new_s, in_sems, out_sems):
    steps = prior_s.shape[0]
    rows = [pl.ds(n * STEP, STEP) for n in range(steps)]
    loads = [pltpu.make_async_copy(state_ref.at[block, rows[n], 0], prior_s.at[n], in_sems.at[n]) for n in range(steps)]
    stores = [pltpu.make_async_copy(new_s.at[n], new_ref.at[block, rows[n], 0], out_sems.at[n]) for n in range(steps)]
    return loads, stores


def recur(block, made, shift_ref, bound_ref, head_ref, loads, stores, prior_s, new_s):
    query, forget_in, value, gate = made
    lower = jax.nn.sigmoid(bound_ref[block : block + 1, :])
    pre = forget_in - shift_ref[block]
    forget = (lower + (1.0 - lower) * jax.nn.sigmoid(pre)).T
    key = ((1.0 - lower) * jax.nn.sigmoid(-pre)).T
    query = query.T
    gate = head_ref[block : block + 1, :] * (gate * jax.nn.sigmoid(gate))
    outs = []
    for n in range(len(loads)):
        loads[n].wait()
        for m in range(STEP):
            at = slice(n * STEP + m, n * STEP + m + 1)
            updated = forget[:, at] * prior_s[n, m] + key[:, at] * value[at, :]
            new_s[n, m] = updated
            outs.append(jnp.sum(query[:, at] * updated, axis=0, keepdims=True))
        stores[n].start()
    readout = jnp.concatenate(outs, axis=0)
    mean = jnp.mean(readout * readout, axis=1, keepdims=True)
    return (readout * lax.rsqrt(mean + epsilon) * gate).astype(jnp.bfloat16)


def first_kernel(share, parts_ref, shift_ref, bound_ref, head_ref, *refs):
    shards, (state_ref, new_ref, out_ref, *scratch) = refs[:-7], refs[-7:]
    loads, stores = moves(0, state_ref, new_ref, *scratch)
    for load in loads:
        load.start()
    owners, _, size = parts_ref.shape
    count = out_ref.shape[1]
    made, squares = [0.0] * 4, 0.0
    for source in range(owners):
        table = parts_ref[source, 4 * count :, :]
        up = jnp.exp2(table[:, 0:1])
        norm = up * 2.0**13
        squares += (table[:, 1:2] + table[:, 2:3]) * norm * norm
        for n in range(4):
            made[n] += parts_ref[source, n * count : (n + 1) * count, :] * up
    scale = lax.rsqrt(squares / D + epsilon)
    made = [scale * total for total in made]
    normed = recur(0, made, shift_ref, bound_ref, head_ref, loads, stores, *scratch[:2])
    width = shards[0].shape[1]
    place = selection(width, size, SHARE_AT, share, True)
    for n, shard in enumerate(shards):
        chunk = lax.rem(lax.axis_index("dp") + n, owners)
        table = parts_ref[chunk, 4 * count :, :]
        branch = jnp.dot(normed, shard[...], preferred_element_type=jnp.float32)
        kept = jnp.dot(table.astype(jnp.bfloat16), place, preferred_element_type=jnp.float32)
        coded = code(branch + jnp.exp2(table[:, 0:1]) * kept)
        for part in range(width // size):
            out_ref[chunk * (width // size) + part] = coded[:, part * size : (part + 1) * size]
    for store in stores:
        store.wait()


def scratch_of(state):
    _, count, _, size, _ = state.shape
    steps = count // STEP
    return [pltpu.VMEM((steps, STEP, size, size), jnp.float32)] * 2 + [pltpu.SemaphoreType.DMA((steps,))] * 2


def first(parts, shift, bound, head, shards, state):
    _, count, _, size, _ = state.shape
    tp = lax.axis_size("tp")
    return pl.pallas_call(
        functools.partial(first_kernel, shards[0].shape[1] // tp),
        in_specs=[VMEM] * (4 + len(shards)) + [HBM],
        out_specs=[HBM, VMEM],
        out_shape=[
            jax.ShapeDtypeStruct(state.shape, jnp.float32),
            jax.ShapeDtypeStruct((tp, count, size), jnp.float32),
        ],
        scratch_shapes=scratch_of(state),
        compiler_params=WIDE_PARAMS,
        name="first",
    )(parts, shift, bound, head, *shards, state)


def decoded(parts_ref):
    parts = parts_ref[...]
    return jnp.sum(parts * jnp.abs(parts), axis=0) * 2.0**-12


def next_kernel(parts_ref, out_ref):
    out_ref[...] = jnp.broadcast_to(decoded(parts_ref).astype(jnp.bfloat16), out_ref.shape)


def second_kernel(share, x_ref, shift_ref, bound_ref, head_ref, *refs):
    shards, (state_ref, _, new_ref, out_ref, *scratch) = refs[:-8], refs[-8:]
    loads, stores = moves(1, state_ref, new_ref, *scratch)
    for load in loads:
        load.start()
    owners, _, size = out_ref.shape
    rows = shards[0].shape[0] - PAD
    parts = rows // size
    count = x_ref.shape[1]
    choose = selection(rows, size, 0, share, False)
    made, squares = 0.0, 0.0
    for n, shard in enumerate(shards):
        chunk = lax.rem(lax.axis_index("dp") + n, owners)
        held = jnp.concatenate([x_ref[chunk * parts + part] for part in range(parts)], axis=1)
        wide = held.astype(jnp.float32)
        squares += jnp.sum(wide * wide, axis=1, keepdims=True)
        gained = (wide * shard[rows : rows + 1, :rows].astype(jnp.float32)).astype(jnp.bfloat16)
        made += jnp.dot(gained, shard[:rows, :], preferred_element_type=jnp.float32)
        kept = jnp.dot(held, choose, preferred_element_type=jnp.float32)
        out_ref[chunk, count:, :] = kept.astype(jnp.bfloat16)
    made = lax.rsqrt(squares / D + epsilon) * made
    made = [made[:, n * size : (n + 1) * size] for n in range(4)]
    normed = recur(1, made, shift_ref, bound_ref, head_ref, loads, stores, *scratch[:2])
    out_ref[:, :count, :] = jnp.broadcast_to(normed, (owners, count, size))
    for store in stores:
        store.wait()


def second(x, shift, bound, head, shards, state, target):
    _, count, _, size, _ = state.shape
    rows = shards[0].shape[0] - PAD
    return pl.pallas_call(
        functools.partial(second_kernel, rows // lax.axis_size("tp")),
        in_specs=[VMEM] * (4 + len(shards)) + [HBM] * 2,
        out_specs=[HBM, VMEM],
        out_shape=[
            jax.ShapeDtypeStruct(state.shape, jnp.float32),
            jax.ShapeDtypeStruct((len(shards), 2 * count, size), jnp.bfloat16),
        ],
        scratch_shapes=scratch_of(state),
        input_output_aliases={5 + len(shards): 0},
        compiler_params=SECOND_PARAMS,
        name="second",
    )(x, shift, bound, head, *shards, state, target)


def branch_kernel(share, normed_ref, w_ref, out_ref):
    count, size = normed_ref.shape[1] // 2, normed_ref.shape[2]
    normed = normed_ref[:, :count, :].reshape(-1, size)
    held = normed_ref[:, count:, :].reshape(-1, size)
    weight = w_ref[1]
    total = jnp.dot(normed, weight, preferred_element_type=jnp.float32)
    place = selection(weight.shape[1], size, 0, share, True)
    total += jnp.dot(held, place, preferred_element_type=jnp.float32)
    out_ref[...] = code(total).reshape(out_ref.shape)


def branch_parts(normed, weight, owners):
    rows = normed.shape[0] * normed.shape[1] // 2 // owners
    return pl.pallas_call(
        functools.partial(branch_kernel, weight.shape[2] // owners),
        out_shape=jax.ShapeDtypeStruct((owners, rows, weight.shape[2]), jnp.float32),
        compiler_params=PARAMS,
        name="branch",
    )(normed, weight)


def final_kernel(parts_ref, out_ref):
    out_ref[...] = decoded(parts_ref)


def layers(
    tokens,
    state,
    lengths,
    norm_gain,
    w_query,
    w_forget,
    w_input,
    w_gate,
    w_out,
    bound_logit,
    pace,
    head_gain,
):
    tp, dp = lax.axis_size("tp"), lax.axis_size("dp")
    whole = exchange(jnp.broadcast_to(tokens, (tp, *tokens.shape)), "tp")
    weights = (w_query, w_forget, w_input, w_gate)
    gain, *firsts = prep(norm_gain, weights)
    back = around(w_out[0], "dp", {})
    whole = after(whole, (back[3], back[dp - 3]))
    log_len = jnp.log(lengths.astype(jnp.float32) / LENGTH_MEAN)
    shift = pace[:, None, :] * log_len[None, :, None]

    message = project(whole, gain, firsts, dp).astype(jnp.float16)
    parts = exchange(message, "dp").astype(jnp.float32)
    target, sums = first(parts, shift, bound_logit, head_gain, back, state)
    held = around(pack(1, after(norm_gain, message), weights), "dp", {2: sums})
    parts = exchange_products(sums, "tp")
    copies = pl.pallas_call(
        next_kernel,
        out_shape=jax.ShapeDtypeStruct(parts.shape, jnp.bfloat16),
        compiler_params=PARAMS,
        name="next",
    )(parts)
    joined = exchange(copies, "tp")
    target, normed = second(joined, shift, bound_logit, head_gain, held, state, target)
    parts = exchange_products(branch_parts(exchange(normed, "dp"), w_out, tp), "tp")
    result = pl.pallas_call(
        final_kernel,
        out_shape=jax.ShapeDtypeStruct(tokens.shape, jnp.float32),
        compiler_params=PARAMS,
        name="final",
    )(parts)
    return result, target


def solution(mesh):
    in_specs = (
        P(("grp", "tp"), "dp"),
        P(None, ("grp", "dp"), "tp", None, None),
        P(("grp", "dp")),
        P(None, "dp"),
        P(None, "dp", "tp"),
        P(None, "dp", "tp"),
        P(None, "dp", "tp"),
        P(None, "dp", "tp"),
        P(None, "tp", "dp"),
        P(None, "tp"),
        P(None, "tp"),
        P(),
    )
    out_specs = (P(("grp", "tp"), "dp"), P(None, ("grp", "dp"), "tp", None, None))
    return jax.shard_map(layers, mesh=mesh, in_specs=in_specs, out_specs=out_specs, check_vma=False)
```

```python
import functools

import jax
import jax.numpy as jnp
from jax import lax
from jax.experimental import pallas as pl
from jax.experimental.pallas import tpu as pltpu
from jax.sharding import PartitionSpec as P


D = 2048
LENGTH_MEAN = 512
FLOOR = 2.0**-80
PAD = 16
LANES = 32
SHARE_AT = 16
STEP = 8
PARAMS = pltpu.CompilerParams(vmem_limit_bytes=16 << 20)
WIDE_PARAMS = pltpu.CompilerParams(vmem_limit_bytes=51 << 20)
PREP_PARAMS = pltpu.CompilerParams(vmem_limit_bytes=54900 << 10)
PACK_PARAMS = pltpu.CompilerParams(vmem_limit_bytes=55300 << 10)
VMEM = pl.BlockSpec(memory_space=pltpu.VMEM)
HBM = pl.BlockSpec(memory_space=pltpu.HBM)

epsilon = 1e-06


def exchange(x, axis):
    return lax.all_to_all(x, axis, split_axis=0, concat_axis=0, tiled=True)


def exchange_products(x, axis):
    return exchange(x.astype(jnp.float16), axis).astype(jnp.float32)


def pack_kernel(block, gain_ref, wq_ref, wf_ref, wi_ref, wg_ref, out_ref, sems):
    rows, size = wq_ref.shape[1:]
    copies = [
        pltpu.make_async_copy(w_ref.at[block], out_ref.at[pl.ds(0, rows), pl.ds(n * size, size)], sems.at[n])
        for n, w_ref in enumerate((wq_ref, wf_ref, wi_ref, wg_ref))
    ]
    for copy in copies:
        copy.start()
    gain = jnp.broadcast_to(gain_ref[block : block + 1, :].astype(jnp.float32), (PAD, rows))
    out_ref[rows:, :rows] = gain.astype(out_ref.dtype)
    out_ref[rows:, rows:] = jnp.zeros((PAD, 4 * size - rows), out_ref.dtype)
    for copy in copies:
        copy.wait()


def pack(block, gain, weights):
    _, rows, size = weights[0].shape
    return pl.pallas_call(
        functools.partial(pack_kernel, block),
        in_specs=[VMEM] + [HBM] * 4,
        out_specs=VMEM,
        out_shape=jax.ShapeDtypeStruct((rows + PAD, 4 * size), jnp.bfloat16),
        scratch_shapes=[pltpu.SemaphoreType.DMA((4,))],
        compiler_params=PACK_PARAMS,
        name="pack",
    )(gain, *weights)


def prep_kernel(gain_ref, *refs):
    weights, row_ref, firsts, sems = refs[:4], refs[4], refs[5:9], refs[9]
    copies = [pltpu.make_async_copy(w_ref.at[0], out, sems.at[n]) for n, (w_ref, out) in enumerate(zip(weights, firsts))]
    for copy in copies:
        copy.start()
    row_ref[...] = gain_ref[0:1, :].astype(jnp.float32)
    for copy in copies:
        copy.wait()


def prep(gain, weights):
    return pl.pallas_call(
        prep_kernel,
        in_specs=[VMEM] + [HBM] * len(weights),
        out_specs=[VMEM] * (1 + len(weights)),
        out_shape=[jax.ShapeDtypeStruct((1, gain.shape[1]), jnp.float32)]
        + [jax.ShapeDtypeStruct(w.shape[1:], w.dtype) for w in weights],
        scratch_shapes=[pltpu.SemaphoreType.DMA((len(weights),))],
        compiler_params=PREP_PARAMS,
        name="prep",
    )(gain, *weights)


def after(x, y):
    return lax.optimization_barrier((x, y))[0]


def side(device):
    return 2 * (device % 2) - 1


def near(shard, axis):
    size = lax.axis_size(axis)
    held = [shard]
    for step in range(1, size // 2):
        pairs = [((n + side(n) * step) % size, n) for n in range(size)]
        held.append(lax.ppermute(shard, axis, pairs))
    return held


def swap(x, axis):
    return lax.ppermute(x, axis, [(n, n ^ 1) for n in range(lax.axis_size(axis))])


def near_chunk(n, owners, device=None):
    device = lax.axis_index("dp") if device is None else device
    return lax.rem(device + (2 * lax.rem(device, 2) - 1) * n + owners, owners)


def selection(rows, columns, start_row, start_column, share):
    row = lax.broadcasted_iota(jnp.int32, (rows, columns), 0) - start_row
    column = lax.broadcasted_iota(jnp.int32, (rows, columns), 1) - start_column
    inside = (row >= 0) & (row < share) & (row == column)
    return jnp.where(inside, 1.0, 0.0).astype(jnp.bfloat16)


def code(total):
    root = jnp.sqrt(jnp.abs(total)) * 2.0**6
    return jnp.where(total < 0.0, -root, root)


def project_kernel(share, x_ref, gain_ref, wq_ref, wf_ref, wi_ref, wg_ref, out_ref):
    owners, size = out_ref.shape[0], out_ref.shape[-1]
    rows = out_ref.shape[1] // 5
    held = x_ref[...].reshape(owners * rows, x_ref.shape[-1])
    x = held.astype(jnp.float32)
    squares = jnp.sum(x * x, axis=1, keepdims=True)
    power = jnp.ceil(0.5 * jnp.log2(jnp.maximum(squares, FLOOR)))
    down = jnp.exp2(-power)
    factor = down * 2.0**13
    gained = (x * gain_ref[...]).astype(jnp.bfloat16)
    for n, w_ref in enumerate((wq_ref, wf_ref, wi_ref, wg_ref)):
        partial = factor * jnp.dot(gained, w_ref[...], preferred_element_type=jnp.float32)
        out_ref[:, n * rows : (n + 1) * rows, :] = partial.reshape(owners, rows, size)
    mantissa = squares * down * down
    high = mantissa.astype(jnp.bfloat16).astype(jnp.float32)
    lane = lax.broadcasted_iota(jnp.int32, (owners * rows, size), 1)
    table = jnp.where(lane == 0, power - 13.0, jnp.where(lane == 1, high, jnp.where(lane == 2, mantissa - high, 0.0)))
    choose = selection(held.shape[1], size, lax.axis_index("tp") * share, SHARE_AT, share)
    kept = factor * jnp.dot(held, choose, preferred_element_type=jnp.float32)
    out_ref[:, 4 * rows :, :] = (table + kept).reshape(owners, rows, size)


def project(whole, gain, weights, owners):
    rows = whole.shape[0] * whole.shape[1] // owners
    share = whole.shape[2] // lax.axis_size("tp")
    return pl.pallas_call(
        functools.partial(project_kernel, share),
        out_shape=jax.ShapeDtypeStruct((owners, 5 * rows, weights[0].shape[1]), jnp.float32),
        compiler_params=PARAMS,
        name="project",
    )(whole, gain, *weights)


def moves(block, state_ref, new_ref, prior_s, new_s, in_sems, out_sems):
    steps = prior_s.shape[0]
    rows = [pl.ds(n * STEP, STEP) for n in range(steps)]
    loads = [pltpu.make_async_copy(state_ref.at[block, rows[n], 0], prior_s.at[n], in_sems.at[n]) for n in range(steps)]
    stores = [pltpu.make_async_copy(new_s.at[n], new_ref.at[block, rows[n], 0], out_sems.at[n]) for n in range(steps)]
    return loads, stores


def recur(block, made, shift_ref, bound_ref, head_ref, loads, stores, prior_s, new_s):
    query, forget_in, value, gate = made
    lower = jax.nn.sigmoid(bound_ref[block : block + 1, :])
    pre = forget_in - shift_ref[block]
    forget = (lower + (1.0 - lower) * jax.nn.sigmoid(pre)).T
    key = ((1.0 - lower) * jax.nn.sigmoid(-pre)).T
    query = query.T
    gate = head_ref[block : block + 1, :] * (gate * jax.nn.sigmoid(gate))
    outs = []
    for n in range(len(loads)):
        loads[n].wait()
        for m in range(STEP):
            at = slice(n * STEP + m, n * STEP + m + 1)
            updated = forget[:, at] * prior_s[n, m] + key[:, at] * value[at, :]
            new_s[n, m] = updated
            outs.append(jnp.sum(query[:, at] * updated, axis=0, keepdims=True))
        stores[n].start()
    readout = jnp.concatenate(outs, axis=0)
    mean = jnp.mean(readout * readout, axis=1, keepdims=True)
    return (readout * lax.rsqrt(mean + epsilon) * gate).astype(jnp.bfloat16)


def first_kernel(share, parts_ref, shift_ref, bound_ref, head_ref, state_ref, new_ref, own_ref, sent_ref, *scratch):
    loads, stores = moves(0, state_ref, new_ref, *scratch)
    for load in loads:
        load.start()
    owners, _, size = parts_ref.shape
    count = shift_ref.shape[1]
    made, squares = [0.0] * 4, 0.0
    for source in range(owners):
        table = parts_ref[source, 4 * count :, :]
        up = jnp.exp2(table[:, 0:1])
        norm = up * 2.0**13
        squares += (table[:, 1:2] + table[:, 2:3]) * norm * norm
        for n in range(4):
            made[n] += parts_ref[source, n * count : (n + 1) * count, :] * up
    scale = lax.rsqrt(squares / D + epsilon)
    made = [scale * total for total in made]
    device = lax.axis_index("dp")
    neighbour = device + 1 - 2 * lax.rem(device, 2)
    for out_ref, holder in ((own_ref, device), (sent_ref, neighbour)):
        kept = 0.0
        for n in range(owners // 2):
            table = parts_ref[near_chunk(n, owners, holder), 4 * count :, :]
            place = selection(size, size, SHARE_AT, n * LANES, share)
            moved = jnp.dot(table.astype(jnp.bfloat16), place, preferred_element_type=jnp.float32)
            kept += jnp.exp2(table[:, 0:1]) * moved
        out_ref[count:, :] = kept.astype(jnp.bfloat16)
    normed = recur(0, made, shift_ref, bound_ref, head_ref, loads, stores, *scratch[:2])
    own_ref[:count, :] = normed
    sent_ref[:count, :] = normed
    for store in stores:
        store.wait()


def pair_kernel(share, own_ref, came_ref, *refs):
    shards, out_ref = refs[:-1], refs[-1]
    count, size = own_ref.shape[0] // 2, own_ref.shape[1]
    normed = jnp.concatenate([own_ref[:count, :], came_ref[:count, :]], axis=0)
    kept = jnp.concatenate([own_ref[count:, :], came_ref[count:, :]], axis=0)
    width = shards[0].shape[1]
    parts = width // size
    blocks = len(shards) * parts
    for n, shard in enumerate(shards):
        place = selection(size, width, n * LANES, lax.axis_index("tp") * share, share)
        total = jnp.dot(normed, shard[...], preferred_element_type=jnp.float32)
        coded = code(total + jnp.dot(kept, place, preferred_element_type=jnp.float32))
        for part in range(parts):
            for half in range(2):
                block = coded[half * count : (half + 1) * count, part * size : (part + 1) * size]
                out_ref[half * blocks + n * parts + part] = block


def pair_parts(own, came, shards):
    tp, size = lax.axis_size("tp"), own.shape[1]
    return pl.pallas_call(
        functools.partial(pair_kernel, shards[0].shape[1] // tp),
        out_shape=jax.ShapeDtypeStruct((tp, own.shape[0] // 2, size), jnp.float32),
        compiler_params=PARAMS,
        name="pair",
    )(own, came, *shards)


def scratch_of(state):
    _, count, _, size, _ = state.shape
    steps = count // STEP
    return [pltpu.VMEM((steps, STEP, size, size), jnp.float32)] * 2 + [pltpu.SemaphoreType.DMA((steps,))] * 2


def first(parts, shift, bound, head, share, state):
    _, count, _, size, _ = state.shape
    sides = jax.ShapeDtypeStruct((2 * count, size), jnp.bfloat16)
    return pl.pallas_call(
        functools.partial(first_kernel, share),
        in_specs=[VMEM] * 4 + [HBM],
        out_specs=[HBM, VMEM, VMEM],
        out_shape=[jax.ShapeDtypeStruct(state.shape, jnp.float32), sides, sides],
        scratch_shapes=scratch_of(state),
        compiler_params=WIDE_PARAMS,
        name="first",
    )(parts, shift, bound, head, state)


def decoded(parts_ref):
    parts = parts_ref[...]
    return jnp.sum(parts * jnp.abs(parts), axis=0) * 2.0**-12


def next_kernel(parts_ref, out_ref):
    out_ref[...] = jnp.broadcast_to(decoded(parts_ref).astype(jnp.bfloat16), out_ref.shape)


def again_kernel(share, x_ref, *refs):
    shards, (own_ref, sent_ref, kept_ref) = refs[:-3], refs[-3:]
    owners, count, size = kept_ref.shape
    rows = shards[0].shape[0] - PAD
    parts = rows // size
    blocks = len(shards) * parts
    kept_ref[...] = jnp.zeros(kept_ref.shape, kept_ref.dtype)
    at = lax.axis_index("tp") * share
    choose = [selection(rows, size, at, half * share, share) for half in range(2)]
    made, squares = 0.0, 0.0
    for n, shard in enumerate(shards):
        halves = []
        for half in range(2):
            first_block = half * blocks + n * parts
            halves.append(jnp.concatenate([x_ref[first_block + part] for part in range(parts)], axis=1))
        held = jnp.concatenate(halves, axis=0)
        wide = held.astype(jnp.float32)
        squares += jnp.sum(wide * wide, axis=1, keepdims=True)
        gained = (wide * shard[rows : rows + 1, :rows].astype(jnp.float32)).astype(jnp.bfloat16)
        made += jnp.dot(gained, shard[:rows, :], preferred_element_type=jnp.float32)
        kept = [jnp.dot(halves[half], choose[half], preferred_element_type=jnp.float32) for half in range(2)]
        kept_ref[near_chunk(n, owners)] = (kept[0] + kept[1]).astype(kept_ref.dtype)
    for half, out_ref in enumerate((own_ref, sent_ref)):
        row = slice(half * count, (half + 1) * count)
        out_ref[:, : made.shape[1]] = made[row]
        out_ref[:, made.shape[1] :] = jnp.broadcast_to(squares[row], (count, size))


def again(x, shards, owners):
    tp, count, size = x.shape
    rows = shards[0].shape[0] - PAD
    sums = jax.ShapeDtypeStruct((count, shards[0].shape[1] + size), jnp.float32)
    return pl.pallas_call(
        functools.partial(again_kernel, rows // tp),
        out_shape=[sums, sums, jax.ShapeDtypeStruct((owners, count, size), jnp.bfloat16)],
        compiler_params=PARAMS,
        name="again",
    )(x, *shards)


def second_kernel(own_ref, came_ref, shift_ref, bound_ref, head_ref, kept_ref, state_ref, _, new_ref, out_ref, *scratch):
    loads, stores = moves(1, state_ref, new_ref, *scratch)
    for load in loads:
        load.start()
    owners, count, size = kept_ref.shape
    total = own_ref[...] + came_ref[...]
    scale = lax.rsqrt(total[:, 4 * size : 4 * size + 1] / D + epsilon)
    made = [scale * total[:, n * size : (n + 1) * size] for n in range(4)]
    out_ref[:, count:, :] = kept_ref[...]
    normed = recur(1, made, shift_ref, bound_ref, head_ref, loads, stores, *scratch[:2])
    out_ref[:, :count, :] = jnp.broadcast_to(normed, (owners, count, size))
    for store in stores:
        store.wait()


def second(own, came, shift, bound, head, kept, state, target):
    owners, count, size = kept.shape
    return pl.pallas_call(
        second_kernel,
        in_specs=[VMEM] * 6 + [HBM] * 2,
        out_specs=[HBM, VMEM],
        out_shape=[
            jax.ShapeDtypeStruct(state.shape, jnp.float32),
            jax.ShapeDtypeStruct((owners, 2 * count, size), jnp.bfloat16),
        ],
        scratch_shapes=scratch_of(state),
        input_output_aliases={7: 0},
        compiler_params=WIDE_PARAMS,
        name="second",
    )(own, came, shift, bound, head, kept, state, target)


def branch_kernel(share, normed_ref, w_ref, out_ref):
    owners, count, size = normed_ref.shape[0], normed_ref.shape[1] // 2, normed_ref.shape[2]
    normed = normed_ref[:, :count, :].reshape(-1, size)
    weight = w_ref[1]
    total = jnp.dot(normed, weight, preferred_element_type=jnp.float32)
    at = lax.axis_index("tp") * share
    mine, other = (selection(size, weight.shape[1], half * share, at, share) for half in range(2))
    flipped = jnp.concatenate([normed_ref[n ^ 1, count:, :] for n in range(owners)], axis=0)
    total += jnp.dot(normed_ref[:, count:, :].reshape(-1, size), mine, preferred_element_type=jnp.float32)
    total += jnp.dot(flipped, other, preferred_element_type=jnp.float32)
    out_ref[...] = code(total).reshape(out_ref.shape)


def branch_parts(normed, weight, owners):
    rows = normed.shape[0] * normed.shape[1] // 2 // owners
    return pl.pallas_call(
        functools.partial(branch_kernel, weight.shape[2] // owners),
        out_shape=jax.ShapeDtypeStruct((owners, rows, weight.shape[2]), jnp.float32),
        compiler_params=PARAMS,
        name="branch",
    )(normed, weight)


def final_kernel(parts_ref, out_ref):
    out_ref[...] = decoded(parts_ref)


def layers(
    tokens,
    state,
    lengths,
    norm_gain,
    w_query,
    w_forget,
    w_input,
    w_gate,
    w_out,
    bound_logit,
    pace,
    head_gain,
):
    tp, dp = lax.axis_size("tp"), lax.axis_size("dp")
    whole = exchange(jnp.broadcast_to(tokens, (tp, *tokens.shape)), "tp")
    weights = (w_query, w_forget, w_input, w_gate)
    gain, *firsts = prep(norm_gain, weights)
    back = near(w_out[0], "dp")
    log_len = jnp.log(lengths.astype(jnp.float32) / LENGTH_MEAN)
    shift = pace[:, None, :] * log_len[None, :, None]

    message = project(whole, gain, firsts, dp).astype(jnp.float16)
    parts = exchange(message, "dp").astype(jnp.float32)
    target, own, sent = first(parts, shift, bound_logit, head_gain, tokens.shape[1] // tp, state)
    held = near(pack(1, norm_gain, weights), "dp")
    came = swap(sent, "dp")
    sums = pair_parts(own, came, back)
    parts = exchange_products(sums, "tp")
    copies = pl.pallas_call(
        next_kernel,
        out_shape=jax.ShapeDtypeStruct(parts.shape, jnp.bfloat16),
        compiler_params=PARAMS,
        name="next",
    )(parts)
    joined = exchange(copies, "tp")
    held = [held[0]] + [after(shard, joined) for shard in held[1:]]
    own, sent, kept = again(joined, held, dp)
    came = swap(sent, "dp")
    target, normed = second(own, came, shift, bound_logit, head_gain, kept, state, target)
    parts = exchange_products(branch_parts(exchange(normed, "dp"), w_out, tp), "tp")
    result = pl.pallas_call(
        final_kernel,
        out_shape=jax.ShapeDtypeStruct(tokens.shape, jnp.float32),
        compiler_params=PARAMS,
        name="final",
    )(parts)
    return result, target


def solution(mesh):
    in_specs = (
        P(("grp", "tp"), "dp"),
        P(None, ("grp", "dp"), "tp", None, None),
        P(("grp", "dp")),
        P(None, "dp"),
        P(None, "dp", "tp"),
        P(None, "dp", "tp"),
        P(None, "dp", "tp"),
        P(None, "dp", "tp"),
        P(None, "tp", "dp"),
        P(None, "tp"),
        P(None, "tp"),
        P(),
    )
    out_specs = (P(("grp", "tp"), "dp"), P(None, ("grp", "dp"), "tp", None, None))
    return jax.shard_map(layers, mesh=mesh, in_specs=in_specs, out_specs=out_specs, check_vma=False)
```

```python
import functools

import jax
import jax.numpy as jnp
from jax import lax
from jax.experimental import pallas as pl
from jax.experimental.pallas import tpu as pltpu
from jax.sharding import PartitionSpec as P


D = 2048
LENGTH_MEAN = 512
FLOOR = 2.0**-80
PAD = 16
LANES = 32
SHARE_AT = 16
STEP = 8
PARAMS = pltpu.CompilerParams(vmem_limit_bytes=16 << 20)
SECOND_PARAMS = pltpu.CompilerParams(vmem_limit_bytes=50 << 20)
LOAD_PARAMS = pltpu.CompilerParams(vmem_limit_bytes=49 << 20)
PREP_PARAMS = pltpu.CompilerParams(vmem_limit_bytes=54900 << 10)
PACK_PARAMS = pltpu.CompilerParams(vmem_limit_bytes=55300 << 10)
VMEM = pl.BlockSpec(memory_space=pltpu.VMEM)
HBM = pl.BlockSpec(memory_space=pltpu.HBM)

epsilon = 1e-06


def exchange(x, axis):
    return lax.all_to_all(x, axis, split_axis=0, concat_axis=0, tiled=True)


def exchange_products(x, axis):
    return exchange(x.astype(jnp.float16), axis).astype(jnp.float32)


def pack_kernel(block, gain_ref, wq_ref, wf_ref, wi_ref, wg_ref, out_ref, sems):
    rows, size = wq_ref.shape[1:]
    copies = [
        pltpu.make_async_copy(w_ref.at[block], out_ref.at[pl.ds(0, rows), pl.ds(n * size, size)], sems.at[n])
        for n, w_ref in enumerate((wq_ref, wf_ref, wi_ref, wg_ref))
    ]
    for copy in copies:
        copy.start()
    gain = jnp.broadcast_to(gain_ref[block : block + 1, :].astype(jnp.float32), (PAD, rows))
    out_ref[rows:, :rows] = gain.astype(out_ref.dtype)
    out_ref[rows:, rows:] = jnp.zeros((PAD, 4 * size - rows), out_ref.dtype)
    for copy in copies:
        copy.wait()


def pack(block, gain, weights):
    _, rows, size = weights[0].shape
    return pl.pallas_call(
        functools.partial(pack_kernel, block),
        in_specs=[VMEM] + [HBM] * 4,
        out_specs=VMEM,
        out_shape=jax.ShapeDtypeStruct((rows + PAD, 4 * size), jnp.bfloat16),
        scratch_shapes=[pltpu.SemaphoreType.DMA((4,))],
        compiler_params=PACK_PARAMS,
        name="pack",
    )(gain, *weights)


def prep_kernel(gain_ref, *refs):
    weights, row_ref, firsts, sems = refs[:4], refs[4], refs[5:9], refs[9]
    copies = [pltpu.make_async_copy(w_ref.at[0], out, sems.at[n]) for n, (w_ref, out) in enumerate(zip(weights, firsts))]
    for copy in copies:
        copy.start()
    row_ref[...] = gain_ref[0:1, :].astype(jnp.float32)
    for copy in copies:
        copy.wait()


def prep(gain, weights):
    return pl.pallas_call(
        prep_kernel,
        in_specs=[VMEM] + [HBM] * len(weights),
        out_specs=[VMEM] * (1 + len(weights)),
        out_shape=[jax.ShapeDtypeStruct((1, gain.shape[1]), jnp.float32)]
        + [jax.ShapeDtypeStruct(w.shape[1:], w.dtype) for w in weights],
        scratch_shapes=[pltpu.SemaphoreType.DMA((len(weights),))],
        compiler_params=PREP_PARAMS,
        name="prep",
    )(gain, *weights)


def after(x, y):
    return lax.optimization_barrier((x, y))[0]


def side(device):
    return 2 * (device % 2) - 1


def near(shard, axis):
    size = lax.axis_size(axis)
    held = [shard]
    for step in range(1, size // 2):
        pairs = [((n + side(n) * step) % size, n) for n in range(size)]
        held.append(lax.ppermute(shard, axis, pairs))
    return held


def swap(x, axis):
    return lax.ppermute(x, axis, [(n, n ^ 1) for n in range(lax.axis_size(axis))])


def near_chunk(n, owners, device=None):
    device = lax.axis_index("dp") if device is None else device
    return lax.rem(device + (2 * lax.rem(device, 2) - 1) * n + owners, owners)


def selection(rows, columns, start_row, start_column, share):
    row = lax.broadcasted_iota(jnp.int32, (rows, columns), 0) - start_row
    column = lax.broadcasted_iota(jnp.int32, (rows, columns), 1) - start_column
    inside = (row >= 0) & (row < share) & (row == column)
    return jnp.where(inside, 1.0, 0.0).astype(jnp.bfloat16)


def code(total):
    root = jnp.sqrt(jnp.abs(total)) * 2.0**6
    return jnp.where(total < 0.0, -root, root)


def project_kernel(share, x_ref, gain_ref, wq_ref, wf_ref, wi_ref, wg_ref, out_ref):
    owners, size = out_ref.shape[0], out_ref.shape[-1]
    rows = out_ref.shape[1] // 5
    held = x_ref[...].reshape(owners * rows, x_ref.shape[-1])
    x = held.astype(jnp.float32)
    squares = jnp.sum(x * x, axis=1, keepdims=True)
    power = jnp.ceil(0.5 * jnp.log2(jnp.maximum(squares, FLOOR)))
    down = jnp.exp2(-power)
    factor = down * 2.0**13
    gained = (x * gain_ref[...]).astype(jnp.bfloat16)
    for n, w_ref in enumerate((wq_ref, wf_ref, wi_ref, wg_ref)):
        partial = factor * jnp.dot(gained, w_ref[...], preferred_element_type=jnp.float32)
        out_ref[:, n * rows : (n + 1) * rows, :] = partial.reshape(owners, rows, size)
    mantissa = squares * down * down
    high = mantissa.astype(jnp.bfloat16).astype(jnp.float32)
    lane = lax.broadcasted_iota(jnp.int32, (owners * rows, size), 1)
    table = jnp.where(lane == 0, power - 13.0, jnp.where(lane == 1, high, jnp.where(lane == 2, mantissa - high, 0.0)))
    choose = selection(held.shape[1], size, lax.axis_index("tp") * share, SHARE_AT, share)
    kept = factor * jnp.dot(held, choose, preferred_element_type=jnp.float32)
    out_ref[:, 4 * rows :, :] = (table + kept).reshape(owners, rows, size)


def project(whole, gain, weights, owners):
    rows = whole.shape[0] * whole.shape[1] // owners
    share = whole.shape[2] // lax.axis_size("tp")
    return pl.pallas_call(
        functools.partial(project_kernel, share),
        out_shape=jax.ShapeDtypeStruct((owners, 5 * rows, weights[0].shape[1]), jnp.float32),
        compiler_params=PARAMS,
        name="project",
    )(whole, gain, *weights)


def store_kernel(new_ref, out_ref, sem):
    copy = pltpu.make_async_copy(new_ref, out_ref.at[0, :, 0], sem)
    copy.start()
    copy.wait()


def store(new, shape):
    return pl.pallas_call(
        store_kernel,
        in_specs=[VMEM],
        out_specs=HBM,
        out_shape=jax.ShapeDtypeStruct(shape, jnp.float32),
        scratch_shapes=[pltpu.SemaphoreType.DMA],
        compiler_params=LOAD_PARAMS,
        name="store",
    )(new)


def recur(block, made, shift_ref, bound_ref, head_ref, prior_ref, new_ref, stores):
    query, forget_in, value, gate = made
    lower = jax.nn.sigmoid(bound_ref[block : block + 1, :])
    pre = forget_in - shift_ref[block]
    forget = (lower + (1.0 - lower) * jax.nn.sigmoid(pre)).T
    key = ((1.0 - lower) * jax.nn.sigmoid(-pre)).T
    query = query.T
    gate = head_ref[block : block + 1, :] * (gate * jax.nn.sigmoid(gate))
    outs = []
    for n in range(value.shape[0]):
        at = slice(n, n + 1)
        updated = forget[:, at] * prior_ref[n] + key[:, at] * value[at, :]
        new_ref[n] = updated
        outs.append(jnp.sum(query[:, at] * updated, axis=0, keepdims=True))
        if stores and n % STEP == STEP - 1:
            stores[n // STEP].start()
    readout = jnp.concatenate(outs, axis=0)
    mean = jnp.mean(readout * readout, axis=1, keepdims=True)
    return (readout * lax.rsqrt(mean + epsilon) * gate).astype(jnp.bfloat16)


def first_kernel(share, parts_ref, shift_ref, bound_ref, head_ref, prior_ref, new_ref, own_ref, sent_ref):
    owners, _, size = parts_ref.shape
    count = shift_ref.shape[1]
    made, squares = [0.0] * 4, 0.0
    for source in range(owners):
        table = parts_ref[source, 4 * count :, :]
        up = jnp.exp2(table[:, 0:1])
        norm = up * 2.0**13
        squares += (table[:, 1:2] + table[:, 2:3]) * norm * norm
        for n in range(4):
            made[n] += parts_ref[source, n * count : (n + 1) * count, :] * up
    scale = lax.rsqrt(squares / D + epsilon)
    made = [scale * total for total in made]
    device = lax.axis_index("dp")
    neighbour = device + 1 - 2 * lax.rem(device, 2)
    for out_ref, holder in ((own_ref, device), (sent_ref, neighbour)):
        kept = 0.0
        for n in range(owners // 2):
            table = parts_ref[near_chunk(n, owners, holder), 4 * count :, :]
            place = selection(size, size, SHARE_AT, n * LANES, share)
            moved = jnp.dot(table.astype(jnp.bfloat16), place, preferred_element_type=jnp.float32)
            kept += jnp.exp2(table[:, 0:1]) * moved
        out_ref[count:, :] = kept.astype(jnp.bfloat16)
    normed = recur(0, made, shift_ref, bound_ref, head_ref, prior_ref, new_ref, ())
    own_ref[:count, :] = normed
    sent_ref[:count, :] = normed


def pair_kernel(share, own_ref, came_ref, *refs):
    shards, out_ref = refs[:-1], refs[-1]
    count, size = own_ref.shape[0] // 2, own_ref.shape[1]
    normed = jnp.concatenate([own_ref[:count, :], came_ref[:count, :]], axis=0)
    kept = jnp.concatenate([own_ref[count:, :], came_ref[count:, :]], axis=0)
    width = shards[0].shape[1]
    parts = width // size
    blocks = len(shards) * parts
    for n, shard in enumerate(shards):
        place = selection(size, width, n * LANES, lax.axis_index("tp") * share, share)
        total = jnp.dot(normed, shard[...], preferred_element_type=jnp.float32)
        coded = code(total + jnp.dot(kept, place, preferred_element_type=jnp.float32))
        for part in range(parts):
            for half in range(2):
                block = coded[half * count : (half + 1) * count, part * size : (part + 1) * size]
                out_ref[half * blocks + n * parts + part] = block


def pair_parts(own, came, shards):
    tp, size = lax.axis_size("tp"), own.shape[1]
    return pl.pallas_call(
        functools.partial(pair_kernel, shards[0].shape[1] // tp),
        out_shape=jax.ShapeDtypeStruct((tp, own.shape[0] // 2, size), jnp.float32),
        compiler_params=PARAMS,
        name="pair",
    )(own, came, *shards)


def first(parts, shift, bound, head, share, prior):
    count, size, _ = prior.shape
    sides = jax.ShapeDtypeStruct((2 * count, size), jnp.bfloat16)
    return pl.pallas_call(
        functools.partial(first_kernel, share),
        out_shape=[jax.ShapeDtypeStruct(prior.shape, jnp.float32), sides, sides],
        compiler_params=PARAMS,
        name="first",
    )(parts, shift, bound, head, prior)


def decoded(parts_ref):
    parts = parts_ref[...]
    return jnp.sum(parts * jnp.abs(parts), axis=0) * 2.0**-12


def next_kernel(parts_ref, out_ref):
    out_ref[...] = jnp.broadcast_to(decoded(parts_ref).astype(jnp.bfloat16), out_ref.shape)


def again_kernel(share, x_ref, *refs):
    shards, (own_ref, sent_ref, kept_ref) = refs[:-3], refs[-3:]
    owners, count, size = kept_ref.shape
    rows = shards[0].shape[0] - PAD
    parts = rows // size
    blocks = len(shards) * parts
    kept_ref[...] = jnp.zeros(kept_ref.shape, kept_ref.dtype)
    at = lax.axis_index("tp") * share
    choose = [selection(rows, size, at, half * share, share) for half in range(2)]
    made, squares = 0.0, 0.0
    for n, shard in enumerate(shards):
        halves = []
        for half in range(2):
            first_block = half * blocks + n * parts
            halves.append(jnp.concatenate([x_ref[first_block + part] for part in range(parts)], axis=1))
        held = jnp.concatenate(halves, axis=0)
        wide = held.astype(jnp.float32)
        squares += jnp.sum(wide * wide, axis=1, keepdims=True)
        gained = (wide * shard[rows : rows + 1, :rows].astype(jnp.float32)).astype(jnp.bfloat16)
        made += jnp.dot(gained, shard[:rows, :], preferred_element_type=jnp.float32)
        kept = [jnp.dot(halves[half], choose[half], preferred_element_type=jnp.float32) for half in range(2)]
        kept_ref[near_chunk(n, owners)] = (kept[0] + kept[1]).astype(kept_ref.dtype)
    for half, out_ref in enumerate((own_ref, sent_ref)):
        row = slice(half * count, (half + 1) * count)
        out_ref[:, : made.shape[1]] = made[row]
        out_ref[:, made.shape[1] :] = jnp.broadcast_to(squares[row], (count, size))


def again(x, shards, owners):
    tp, count, size = x.shape
    rows = shards[0].shape[0] - PAD
    sums = jax.ShapeDtypeStruct((count, shards[0].shape[1] + size), jnp.float32)
    return pl.pallas_call(
        functools.partial(again_kernel, rows // tp),
        out_shape=[sums, sums, jax.ShapeDtypeStruct((owners, count, size), jnp.bfloat16)],
        compiler_params=PARAMS,
        name="again",
    )(x, *shards)


def second_kernel(own_ref, came_ref, shift_ref, bound_ref, head_ref, kept_ref, prior_ref, _, new_ref, out_ref, new_s, sems):
    owners, count, size = kept_ref.shape
    stores = []
    for n in range(count // STEP):
        rows = pl.ds(n * STEP, STEP)
        stores.append(pltpu.make_async_copy(new_s.at[rows], new_ref.at[1, rows, 0], sems.at[n]))
    total = own_ref[...] + came_ref[...]
    scale = lax.rsqrt(total[:, 4 * size : 4 * size + 1] / D + epsilon)
    made = [scale * total[:, n * size : (n + 1) * size] for n in range(4)]
    out_ref[:, count:, :] = kept_ref[...]
    normed = recur(1, made, shift_ref, bound_ref, head_ref, prior_ref, new_s, stores)
    out_ref[:, :count, :] = jnp.broadcast_to(normed, (owners, count, size))
    for store in stores:
        store.wait()


def second(own, came, shift, bound, head, kept, prior, target):
    owners, count, size = kept.shape
    return pl.pallas_call(
        second_kernel,
        in_specs=[VMEM] * 7 + [HBM],
        out_specs=[HBM, VMEM],
        out_shape=[
            jax.ShapeDtypeStruct(target.shape, jnp.float32),
            jax.ShapeDtypeStruct((owners, 2 * count, size), jnp.bfloat16),
        ],
        scratch_shapes=[pltpu.VMEM(prior.shape, jnp.float32), pltpu.SemaphoreType.DMA((count // STEP,))],
        input_output_aliases={7: 0},
        compiler_params=SECOND_PARAMS,
        name="second",
    )(own, came, shift, bound, head, kept, prior, target)


def branch_kernel(share, normed_ref, w_ref, out_ref):
    owners, count, size = normed_ref.shape[0], normed_ref.shape[1] // 2, normed_ref.shape[2]
    normed = normed_ref[:, :count, :].reshape(-1, size)
    weight = w_ref[1]
    total = jnp.dot(normed, weight, preferred_element_type=jnp.float32)
    at = lax.axis_index("tp") * share
    mine, other = (selection(size, weight.shape[1], half * share, at, share) for half in range(2))
    flipped = jnp.concatenate([normed_ref[n ^ 1, count:, :] for n in range(owners)], axis=0)
    total += jnp.dot(normed_ref[:, count:, :].reshape(-1, size), mine, preferred_element_type=jnp.float32)
    total += jnp.dot(flipped, other, preferred_element_type=jnp.float32)
    out_ref[...] = code(total).reshape(out_ref.shape)


def branch_parts(normed, weight, owners):
    rows = normed.shape[0] * normed.shape[1] // 2 // owners
    return pl.pallas_call(
        functools.partial(branch_kernel, weight.shape[2] // owners),
        out_shape=jax.ShapeDtypeStruct((owners, rows, weight.shape[2]), jnp.float32),
        compiler_params=PARAMS,
        name="branch",
    )(normed, weight)


def final_kernel(parts_ref, out_ref):
    out_ref[...] = decoded(parts_ref)


def layers(
    tokens,
    state,
    lengths,
    norm_gain,
    w_query,
    w_forget,
    w_input,
    w_gate,
    w_out,
    bound_logit,
    pace,
    head_gain,
):
    tp, dp = lax.axis_size("tp"), lax.axis_size("dp")
    whole = exchange(jnp.broadcast_to(tokens, (tp, *tokens.shape)), "tp")
    weights = (w_query, w_forget, w_input, w_gate)
    gain, *firsts = prep(norm_gain, weights)
    back = near(w_out[0], "dp")
    log_len = jnp.log(lengths.astype(jnp.float32) / LENGTH_MEAN)
    shift = pace[:, None, :] * log_len[None, :, None]

    message = project(whole, gain, firsts, dp).astype(jnp.float16)
    parts = exchange(message, "dp").astype(jnp.float32)
    new, own, sent = first(
        parts, shift, bound_logit, head_gain, tokens.shape[1] // tp, after(state, message)[0, :, 0]
    )
    held = near(pack(1, norm_gain, weights), "dp")
    came = swap(sent, "dp")
    sums = pair_parts(own, came, back)
    parts = exchange_products(sums, "tp")
    copies = pl.pallas_call(
        next_kernel,
        out_shape=jax.ShapeDtypeStruct(parts.shape, jnp.bfloat16),
        compiler_params=PARAMS,
        name="next",
    )(parts)
    joined = exchange(copies, "tp")
    prior = after(state, copies)[1, :, 0]
    target = store(after(new, sums), state.shape)
    held = [held[0]] + [after(shard, joined) for shard in held[1:]]
    own, sent, kept = again(joined, held, dp)
    came = swap(sent, "dp")
    target, normed = second(own, came, shift, bound_logit, head_gain, kept, prior, target)
    parts = exchange_products(branch_parts(exchange(normed, "dp"), w_out, tp), "tp")
    result = pl.pallas_call(
        final_kernel,
        out_shape=jax.ShapeDtypeStruct(tokens.shape, jnp.float32),
        compiler_params=PARAMS,
        name="final",
    )(parts)
    return result, target


def solution(mesh):
    in_specs = (
        P(("grp", "tp"), "dp"),
        P(None, ("grp", "dp"), "tp", None, None),
        P(("grp", "dp")),
        P(None, "dp"),
        P(None, "dp", "tp"),
        P(None, "dp", "tp"),
        P(None, "dp", "tp"),
        P(None, "dp", "tp"),
        P(None, "tp", "dp"),
        P(None, "tp"),
        P(None, "tp"),
        P(),
    )
    out_specs = (P(("grp", "tp"), "dp"), P(None, ("grp", "dp"), "tp", None, None))
    return jax.shard_map(layers, mesh=mesh, in_specs=in_specs, out_specs=out_specs, check_vma=False)
```

```python
import functools

import jax
import jax.numpy as jnp
from jax import lax
from jax.experimental import pallas as pl
from jax.experimental.pallas import tpu as pltpu
from jax.sharding import PartitionSpec as P


D = 2048
LENGTH_MEAN = 512
FLOOR = 2.0**-80
PAD = 16
LANES = 32
SHARE_AT = 16
STEP = 4
AHEAD = 3
PARAMS = pltpu.CompilerParams(vmem_limit_bytes=16 << 20)
SECOND_PARAMS = pltpu.CompilerParams(vmem_limit_bytes=50 << 20)
WIDE_PARAMS = pltpu.CompilerParams(vmem_limit_bytes=51 << 20)
PREP_PARAMS = pltpu.CompilerParams(vmem_limit_bytes=54900 << 10)
PACK_PARAMS = pltpu.CompilerParams(vmem_limit_bytes=55300 << 10)
VMEM = pl.BlockSpec(memory_space=pltpu.VMEM)
HBM = pl.BlockSpec(memory_space=pltpu.HBM)

epsilon = 1e-06


def exchange(x, axis):
    return lax.all_to_all(x, axis, split_axis=0, concat_axis=0, tiled=True)


def exchange_products(x, axis):
    return exchange(x.astype(jnp.float16), axis).astype(jnp.float32)


def pack_kernel(block, gain_ref, wq_ref, wf_ref, wi_ref, wg_ref, out_ref, sems):
    rows, size = wq_ref.shape[1:]
    copies = [
        pltpu.make_async_copy(w_ref.at[block], out_ref.at[pl.ds(0, rows), pl.ds(n * size, size)], sems.at[n])
        for n, w_ref in enumerate((wq_ref, wf_ref, wi_ref, wg_ref))
    ]
    for copy in copies:
        copy.start()
    gain = jnp.broadcast_to(gain_ref[block : block + 1, :].astype(jnp.float32), (PAD, rows))
    out_ref[rows:, :rows] = gain.astype(out_ref.dtype)
    out_ref[rows:, rows:] = jnp.zeros((PAD, 4 * size - rows), out_ref.dtype)
    for copy in copies:
        copy.wait()


def pack(block, gain, weights):
    _, rows, size = weights[0].shape
    return pl.pallas_call(
        functools.partial(pack_kernel, block),
        in_specs=[VMEM] + [HBM] * 4,
        out_specs=VMEM,
        out_shape=jax.ShapeDtypeStruct((rows + PAD, 4 * size), jnp.bfloat16),
        scratch_shapes=[pltpu.SemaphoreType.DMA((4,))],
        compiler_params=PACK_PARAMS,
        name="pack",
    )(gain, *weights)


def prep_kernel(gain_ref, *refs):
    weights, row_ref, firsts, sems = refs[:4], refs[4], refs[5:9], refs[9]
    copies = [pltpu.make_async_copy(w_ref.at[0], out, sems.at[n]) for n, (w_ref, out) in enumerate(zip(weights, firsts))]
    for copy in copies:
        copy.start()
    row_ref[...] = gain_ref[0:1, :].astype(jnp.float32)
    for copy in copies:
        copy.wait()


def prep(gain, weights):
    return pl.pallas_call(
        prep_kernel,
        in_specs=[VMEM] + [HBM] * len(weights),
        out_specs=[VMEM] * (1 + len(weights)),
        out_shape=[jax.ShapeDtypeStruct((1, gain.shape[1]), jnp.float32)]
        + [jax.ShapeDtypeStruct(w.shape[1:], w.dtype) for w in weights],
        scratch_shapes=[pltpu.SemaphoreType.DMA((len(weights),))],
        compiler_params=PREP_PARAMS,
        name="prep",
    )(gain, *weights)


def after(x, y):
    return lax.optimization_barrier((x, y))[0]


def side(device):
    return 2 * (device % 2) - 1


def near(shard, axis):
    size = lax.axis_size(axis)
    held = [shard]
    for step in range(1, size // 2):
        pairs = [((n + side(n) * step) % size, n) for n in range(size)]
        held.append(lax.ppermute(shard, axis, pairs))
    return held


def swap(x, axis):
    return lax.ppermute(x, axis, [(n, n ^ 1) for n in range(lax.axis_size(axis))])


def near_chunk(n, owners, device=None):
    device = lax.axis_index("dp") if device is None else device
    return lax.rem(device + (2 * lax.rem(device, 2) - 1) * n + owners, owners)


def selection(rows, columns, start_row, start_column, share):
    row = lax.broadcasted_iota(jnp.int32, (rows, columns), 0) - start_row
    column = lax.broadcasted_iota(jnp.int32, (rows, columns), 1) - start_column
    inside = (row >= 0) & (row < share) & (row == column)
    return jnp.where(inside, 1.0, 0.0).astype(jnp.bfloat16)


def code(total):
    root = jnp.sqrt(jnp.abs(total)) * 2.0**6
    return jnp.where(total < 0.0, -root, root)


def project_kernel(share, x_ref, gain_ref, wq_ref, wf_ref, wi_ref, wg_ref, out_ref):
    owners, size = out_ref.shape[0], out_ref.shape[-1]
    rows = out_ref.shape[1] // 5
    held = x_ref[...].reshape(owners * rows, x_ref.shape[-1])
    x = held.astype(jnp.float32)
    squares = jnp.sum(x * x, axis=1, keepdims=True)
    power = jnp.ceil(0.5 * jnp.log2(jnp.maximum(squares, FLOOR)))
    down = jnp.exp2(-power)
    factor = down * 2.0**13
    gained = (x * gain_ref[...]).astype(jnp.bfloat16)
    for n, w_ref in enumerate((wq_ref, wf_ref, wi_ref, wg_ref)):
        partial = factor * jnp.dot(gained, w_ref[...], preferred_element_type=jnp.float32)
        out_ref[:, n * rows : (n + 1) * rows, :] = partial.reshape(owners, rows, size)
    mantissa = squares * down * down
    high = mantissa.astype(jnp.bfloat16).astype(jnp.float32)
    lane = lax.broadcasted_iota(jnp.int32, (owners * rows, size), 1)
    table = jnp.where(lane == 0, power - 13.0, jnp.where(lane == 1, high, jnp.where(lane == 2, mantissa - high, 0.0)))
    choose = selection(held.shape[1], size, lax.axis_index("tp") * share, SHARE_AT, share)
    kept = factor * jnp.dot(held, choose, preferred_element_type=jnp.float32)
    out_ref[:, 4 * rows :, :] = (table + kept).reshape(owners, rows, size)


def project(whole, gain, weights, owners):
    rows = whole.shape[0] * whole.shape[1] // owners
    share = whole.shape[2] // lax.axis_size("tp")
    return pl.pallas_call(
        functools.partial(project_kernel, share),
        out_shape=jax.ShapeDtypeStruct((owners, 5 * rows, weights[0].shape[1]), jnp.float32),
        compiler_params=PARAMS,
        name="project",
    )(whole, gain, *weights)


def recur(block, made, shift_ref, bound_ref, head_ref, prior_ref, new_ref, loads, stores):
    query, forget_in, value, gate = made
    lower = jax.nn.sigmoid(bound_ref[block : block + 1, :])
    pre = forget_in - shift_ref[block]
    forget = (lower + (1.0 - lower) * jax.nn.sigmoid(pre)).T
    key = ((1.0 - lower) * jax.nn.sigmoid(-pre)).T
    query = query.T
    gate = head_ref[block : block + 1, :] * (gate * jax.nn.sigmoid(gate))
    outs = []
    for n in range(value.shape[0]):
        if loads and n % STEP == 0:
            loads[n // STEP].wait()
            if n // STEP + AHEAD < len(loads):
                loads[n // STEP + AHEAD].start()
        at = slice(n, n + 1)
        updated = forget[:, at] * prior_ref[n] + key[:, at] * value[at, :]
        new_ref[n] = updated
        outs.append(jnp.sum(query[:, at] * updated, axis=0, keepdims=True))
        if n % STEP == STEP - 1:
            stores[n // STEP].start()
    readout = jnp.concatenate(outs, axis=0)
    mean = jnp.mean(readout * readout, axis=1, keepdims=True)
    return (readout * lax.rsqrt(mean + epsilon) * gate).astype(jnp.bfloat16)


def first_kernel(share, parts_ref, shift_ref, bound_ref, head_ref, state_ref, new_ref, own_ref, sent_ref, *scratch):
    prior_s, new_s, in_sems, out_sems = scratch
    loads, stores = [], []
    for n in range(shift_ref.shape[1] // STEP):
        rows = pl.ds(n * STEP, STEP)
        loads.append(pltpu.make_async_copy(state_ref.at[0, rows, 0], prior_s.at[rows], in_sems.at[n]))
        stores.append(pltpu.make_async_copy(new_s.at[rows], new_ref.at[0, rows, 0], out_sems.at[n]))
    for load in loads[:AHEAD]:
        load.start()
    owners, _, size = parts_ref.shape
    count = shift_ref.shape[1]
    made, squares = [0.0] * 4, 0.0
    for source in range(owners):
        table = parts_ref[source, 4 * count :, :]
        up = jnp.exp2(table[:, 0:1])
        norm = up * 2.0**13
        squares += (table[:, 1:2] + table[:, 2:3]) * norm * norm
        for n in range(4):
            made[n] += parts_ref[source, n * count : (n + 1) * count, :] * up
    scale = lax.rsqrt(squares / D + epsilon)
    made = [scale * total for total in made]
    device = lax.axis_index("dp")
    neighbour = device + 1 - 2 * lax.rem(device, 2)
    for out_ref, holder in ((own_ref, device), (sent_ref, neighbour)):
        kept = 0.0
        for n in range(owners // 2):
            table = parts_ref[near_chunk(n, owners, holder), 4 * count :, :]
            place = selection(size, size, SHARE_AT, n * LANES, share)
            moved = jnp.dot(table.astype(jnp.bfloat16), place, preferred_element_type=jnp.float32)
            kept += jnp.exp2(table[:, 0:1]) * moved
        out_ref[count:, :] = kept.astype(jnp.bfloat16)
    normed = recur(0, made, shift_ref, bound_ref, head_ref, prior_s, new_s, loads, stores)
    own_ref[:count, :] = normed
    sent_ref[:count, :] = normed
    for store in stores:
        store.wait()


def pair_kernel(share, own_ref, came_ref, *refs):
    shards, out_ref = refs[:-1], refs[-1]
    count, size = own_ref.shape[0] // 2, own_ref.shape[1]
    normed = jnp.concatenate([own_ref[:count, :], came_ref[:count, :]], axis=0)
    kept = jnp.concatenate([own_ref[count:, :], came_ref[count:, :]], axis=0)
    width = shards[0].shape[1]
    parts = width // size
    blocks = len(shards) * parts
    for n, shard in enumerate(shards):
        place = selection(size, width, n * LANES, lax.axis_index("tp") * share, share)
        total = jnp.dot(normed, shard[...], preferred_element_type=jnp.float32)
        coded = code(total + jnp.dot(kept, place, preferred_element_type=jnp.float32))
        for part in range(parts):
            for half in range(2):
                block = coded[half * count : (half + 1) * count, part * size : (part + 1) * size]
                out_ref[half * blocks + n * parts + part] = block


def pair_parts(own, came, shards):
    tp, size = lax.axis_size("tp"), own.shape[1]
    return pl.pallas_call(
        functools.partial(pair_kernel, shards[0].shape[1] // tp),
        out_shape=jax.ShapeDtypeStruct((tp, own.shape[0] // 2, size), jnp.float32),
        compiler_params=PARAMS,
        name="pair",
    )(own, came, *shards)


def first(parts, shift, bound, head, share, state):
    _, count, _, size, _ = state.shape
    sides = jax.ShapeDtypeStruct((2 * count, size), jnp.bfloat16)
    return pl.pallas_call(
        functools.partial(first_kernel, share),
        in_specs=[VMEM] * 4 + [HBM],
        out_specs=[HBM, VMEM, VMEM],
        out_shape=[jax.ShapeDtypeStruct(state.shape, jnp.float32), sides, sides],
        scratch_shapes=[pltpu.VMEM((count, size, size), jnp.float32)] * 2
        + [pltpu.SemaphoreType.DMA((count // STEP,))] * 2,
        compiler_params=WIDE_PARAMS,
        name="first",
    )(parts, shift, bound, head, state)


def decoded(parts_ref):
    parts = parts_ref[...]
    return jnp.sum(parts * jnp.abs(parts), axis=0) * 2.0**-12


def next_kernel(parts_ref, out_ref):
    out_ref[...] = jnp.broadcast_to(decoded(parts_ref).astype(jnp.bfloat16), out_ref.shape)


def again_kernel(share, x_ref, *refs):
    shards, (own_ref, sent_ref, kept_ref) = refs[:-3], refs[-3:]
    owners, count, size = kept_ref.shape
    rows = shards[0].shape[0] - PAD
    parts = rows // size
    blocks = len(shards) * parts
    kept_ref[...] = jnp.zeros(kept_ref.shape, kept_ref.dtype)
    at = lax.axis_index("tp") * share
    choose = [selection(rows, size, at, half * share, share) for half in range(2)]
    made, squares = 0.0, 0.0
    for n, shard in enumerate(shards):
        halves = []
        for half in range(2):
            first_block = half * blocks + n * parts
            halves.append(jnp.concatenate([x_ref[first_block + part] for part in range(parts)], axis=1))
        held = jnp.concatenate(halves, axis=0)
        wide = held.astype(jnp.float32)
        squares += jnp.sum(wide * wide, axis=1, keepdims=True)
        gained = (wide * shard[rows : rows + 1, :rows].astype(jnp.float32)).astype(jnp.bfloat16)
        made += jnp.dot(gained, shard[:rows, :], preferred_element_type=jnp.float32)
        kept = [jnp.dot(halves[half], choose[half], preferred_element_type=jnp.float32) for half in range(2)]
        kept_ref[near_chunk(n, owners)] = (kept[0] + kept[1]).astype(kept_ref.dtype)
    for half, out_ref in enumerate((own_ref, sent_ref)):
        row = slice(half * count, (half + 1) * count)
        out_ref[:, : made.shape[1]] = made[row]
        out_ref[:, made.shape[1] :] = jnp.broadcast_to(squares[row], (count, size))


def again(x, shards, owners):
    tp, count, size = x.shape
    rows = shards[0].shape[0] - PAD
    sums = jax.ShapeDtypeStruct((count, shards[0].shape[1] + size), jnp.float32)
    return pl.pallas_call(
        functools.partial(again_kernel, rows // tp),
        out_shape=[sums, sums, jax.ShapeDtypeStruct((owners, count, size), jnp.bfloat16)],
        compiler_params=PARAMS,
        name="again",
    )(x, *shards)


def second_kernel(own_ref, came_ref, shift_ref, bound_ref, head_ref, kept_ref, prior_ref, _, new_ref, out_ref, new_s, sems):
    owners, count, size = kept_ref.shape
    stores = []
    for n in range(count // STEP):
        rows = pl.ds(n * STEP, STEP)
        stores.append(pltpu.make_async_copy(new_s.at[rows], new_ref.at[1, rows, 0], sems.at[n]))
    total = own_ref[...] + came_ref[...]
    scale = lax.rsqrt(total[:, 4 * size : 4 * size + 1] / D + epsilon)
    made = [scale * total[:, n * size : (n + 1) * size] for n in range(4)]
    out_ref[:, count:, :] = kept_ref[...]
    normed = recur(1, made, shift_ref, bound_ref, head_ref, prior_ref, new_s, (), stores)
    out_ref[:, :count, :] = jnp.broadcast_to(normed, (owners, count, size))
    for store in stores:
        store.wait()


def second(own, came, shift, bound, head, kept, prior, target):
    owners, count, size = kept.shape
    return pl.pallas_call(
        second_kernel,
        in_specs=[VMEM] * 7 + [HBM],
        out_specs=[HBM, VMEM],
        out_shape=[
            jax.ShapeDtypeStruct(target.shape, jnp.float32),
            jax.ShapeDtypeStruct((owners, 2 * count, size), jnp.bfloat16),
        ],
        scratch_shapes=[pltpu.VMEM(prior.shape, jnp.float32), pltpu.SemaphoreType.DMA((count // STEP,))],
        input_output_aliases={7: 0},
        compiler_params=SECOND_PARAMS,
        name="second",
    )(own, came, shift, bound, head, kept, prior, target)


def branch_kernel(share, normed_ref, w_ref, out_ref):
    owners, count, size = normed_ref.shape[0], normed_ref.shape[1] // 2, normed_ref.shape[2]
    normed = normed_ref[:, :count, :].reshape(-1, size)
    weight = w_ref[1]
    total = jnp.dot(normed, weight, preferred_element_type=jnp.float32)
    at = lax.axis_index("tp") * share
    mine, other = (selection(size, weight.shape[1], half * share, at, share) for half in range(2))
    flipped = jnp.concatenate([normed_ref[n ^ 1, count:, :] for n in range(owners)], axis=0)
    total += jnp.dot(normed_ref[:, count:, :].reshape(-1, size), mine, preferred_element_type=jnp.float32)
    total += jnp.dot(flipped, other, preferred_element_type=jnp.float32)
    out_ref[...] = code(total).reshape(out_ref.shape)


def branch_parts(normed, weight, owners):
    rows = normed.shape[0] * normed.shape[1] // 2 // owners
    return pl.pallas_call(
        functools.partial(branch_kernel, weight.shape[2] // owners),
        out_shape=jax.ShapeDtypeStruct((owners, rows, weight.shape[2]), jnp.float32),
        compiler_params=PARAMS,
        name="branch",
    )(normed, weight)


def final_kernel(parts_ref, out_ref):
    out_ref[...] = decoded(parts_ref)


def layers(
    tokens,
    state,
    lengths,
    norm_gain,
    w_query,
    w_forget,
    w_input,
    w_gate,
    w_out,
    bound_logit,
    pace,
    head_gain,
):
    tp, dp = lax.axis_size("tp"), lax.axis_size("dp")
    whole = exchange(jnp.broadcast_to(tokens, (tp, *tokens.shape)), "tp")
    weights = (w_query, w_forget, w_input, w_gate)
    gain, *firsts = prep(norm_gain, weights)
    back = near(w_out[0], "dp")
    log_len = jnp.log(lengths.astype(jnp.float32) / LENGTH_MEAN)
    shift = pace[:, None, :] * log_len[None, :, None]

    message = project(whole, gain, firsts, dp).astype(jnp.float16)
    parts = exchange(message, "dp").astype(jnp.float32)
    target, own, sent = first(parts, shift, bound_logit, head_gain, tokens.shape[1] // tp, state)
    held = near(pack(1, norm_gain, weights), "dp")
    came = swap(sent, "dp")
    sums = pair_parts(own, came, back)
    parts = exchange_products(sums, "tp")
    copies = pl.pallas_call(
        next_kernel,
        out_shape=jax.ShapeDtypeStruct(parts.shape, jnp.bfloat16),
        compiler_params=PARAMS,
        name="next",
    )(parts)
    joined = exchange(after(copies, held[1:]), "tp")
    prior = after(state, joined)[1, :, 0]
    own, sent, kept = again(joined, held, dp)
    came = swap(sent, "dp")
    target, normed = second(own, came, shift, bound_logit, head_gain, kept, prior, target)
    parts = exchange_products(branch_parts(exchange(normed, "dp"), w_out, tp), "tp")
    result = pl.pallas_call(
        final_kernel,
        out_shape=jax.ShapeDtypeStruct(tokens.shape, jnp.float32),
        compiler_params=PARAMS,
        name="final",
    )(parts)
    return result, target


def solution(mesh):
    in_specs = (
        P(("grp", "tp"), "dp"),
        P(None, ("grp", "dp"), "tp", None, None),
        P(("grp", "dp")),
        P(None, "dp"),
        P(None, "dp", "tp"),
        P(None, "dp", "tp"),
        P(None, "dp", "tp"),
        P(None, "dp", "tp"),
        P(None, "tp", "dp"),
        P(None, "tp"),
        P(None, "tp"),
        P(),
    )
    out_specs = (P(("grp", "tp"), "dp"), P(None, ("grp", "dp"), "tp", None, None))
    return jax.shard_map(layers, mesh=mesh, in_specs=in_specs, out_specs=out_specs, check_vma=False)
```

```python
import functools

import jax
import jax.numpy as jnp
from jax import lax
from jax.experimental import pallas as pl
from jax.experimental.pallas import tpu as pltpu
from jax.sharding import PartitionSpec as P


D = 2048
LENGTH_MEAN = 512
FLOOR = 2.0**-80
PAD = 16
LANES = 32
SHARE_AT = 16
STEP = 8
PARAMS = pltpu.CompilerParams(vmem_limit_bytes=16 << 20)
SECOND_PARAMS = pltpu.CompilerParams(vmem_limit_bytes=50 << 20)
WIDE_PARAMS = pltpu.CompilerParams(vmem_limit_bytes=51 << 20)
PREP_PARAMS = pltpu.CompilerParams(vmem_limit_bytes=54900 << 10)
PACK_PARAMS = pltpu.CompilerParams(vmem_limit_bytes=55300 << 10)
VMEM = pl.BlockSpec(memory_space=pltpu.VMEM)
HBM = pl.BlockSpec(memory_space=pltpu.HBM)

epsilon = 1e-06


def exchange(x, axis):
    return lax.all_to_all(x, axis, split_axis=0, concat_axis=0, tiled=True)


def exchange_products(x, axis):
    return exchange(x.astype(jnp.float16), axis).astype(jnp.float32)


def pack_kernel(block, gain_ref, wq_ref, wf_ref, wi_ref, wg_ref, out_ref, sems):
    rows, size = wq_ref.shape[1:]
    copies = [
        pltpu.make_async_copy(w_ref.at[block], out_ref.at[pl.ds(0, rows), pl.ds(n * size, size)], sems.at[n])
        for n, w_ref in enumerate((wq_ref, wf_ref, wi_ref, wg_ref))
    ]
    for copy in copies:
        copy.start()
    gain = jnp.broadcast_to(gain_ref[block : block + 1, :].astype(jnp.float32), (PAD, rows))
    out_ref[rows:, :rows] = gain.astype(out_ref.dtype)
    out_ref[rows:, rows:] = jnp.zeros((PAD, 4 * size - rows), out_ref.dtype)
    for copy in copies:
        copy.wait()


def pack(block, gain, weights):
    _, rows, size = weights[0].shape
    return pl.pallas_call(
        functools.partial(pack_kernel, block),
        in_specs=[VMEM] + [HBM] * 4,
        out_specs=VMEM,
        out_shape=jax.ShapeDtypeStruct((rows + PAD, 4 * size), jnp.bfloat16),
        scratch_shapes=[pltpu.SemaphoreType.DMA((4,))],
        compiler_params=PACK_PARAMS,
        name="pack",
    )(gain, *weights)


def prep_kernel(gain_ref, *refs):
    weights, row_ref, firsts, sems = refs[:4], refs[4], refs[5:9], refs[9]
    copies = [pltpu.make_async_copy(w_ref.at[0], out, sems.at[n]) for n, (w_ref, out) in enumerate(zip(weights, firsts))]
    for copy in copies:
        copy.start()
    row_ref[...] = gain_ref[0:1, :].astype(jnp.float32)
    for copy in copies:
        copy.wait()


def prep(gain, weights):
    return pl.pallas_call(
        prep_kernel,
        in_specs=[VMEM] + [HBM] * len(weights),
        out_specs=[VMEM] * (1 + len(weights)),
        out_shape=[jax.ShapeDtypeStruct((1, gain.shape[1]), jnp.float32)]
        + [jax.ShapeDtypeStruct(w.shape[1:], w.dtype) for w in weights],
        scratch_shapes=[pltpu.SemaphoreType.DMA((len(weights),))],
        compiler_params=PREP_PARAMS,
        name="prep",
    )(gain, *weights)


def after(x, y):
    return lax.optimization_barrier((x, y))[0]


def side(device):
    return 2 * (device % 2) - 1


def near(shard, axis):
    size = lax.axis_size(axis)
    held = [shard]
    for step in range(1, size // 2):
        pairs = [((n + side(n) * step) % size, n) for n in range(size)]
        held.append(lax.ppermute(shard, axis, pairs))
    return held


def swap(x, axis):
    return lax.ppermute(x, axis, [(n, n ^ 1) for n in range(lax.axis_size(axis))])


def near_chunk(n, owners, device=None):
    device = lax.axis_index("dp") if device is None else device
    return lax.rem(device + (2 * lax.rem(device, 2) - 1) * n + owners, owners)


def selection(rows, columns, start_row, start_column, share):
    row = lax.broadcasted_iota(jnp.int32, (rows, columns), 0) - start_row
    column = lax.broadcasted_iota(jnp.int32, (rows, columns), 1) - start_column
    inside = (row >= 0) & (row < share) & (row == column)
    return jnp.where(inside, 1.0, 0.0).astype(jnp.bfloat16)


def code(total):
    root = jnp.sqrt(jnp.abs(total)) * 2.0**6
    return jnp.where(total < 0.0, -root, root)


def project_kernel(share, x_ref, gain_ref, wq_ref, wf_ref, wi_ref, wg_ref, out_ref):
    owners, size = out_ref.shape[0], out_ref.shape[-1]
    rows = out_ref.shape[1] // 5
    held = x_ref[...].reshape(owners * rows, x_ref.shape[-1])
    x = held.astype(jnp.float32)
    squares = jnp.sum(x * x, axis=1, keepdims=True)
    power = jnp.ceil(0.5 * jnp.log2(jnp.maximum(squares, FLOOR)))
    down = jnp.exp2(-power)
    factor = down * 2.0**13
    gained = (x * gain_ref[...]).astype(jnp.bfloat16)
    for n, w_ref in enumerate((wq_ref, wf_ref, wi_ref, wg_ref)):
        partial = factor * jnp.dot(gained, w_ref[...], preferred_element_type=jnp.float32)
        out_ref[:, n * rows : (n + 1) * rows, :] = partial.reshape(owners, rows, size)
    mantissa = squares * down * down
    high = mantissa.astype(jnp.bfloat16).astype(jnp.float32)
    lane = lax.broadcasted_iota(jnp.int32, (owners * rows, size), 1)
    table = jnp.where(lane == 0, power - 13.0, jnp.where(lane == 1, high, jnp.where(lane == 2, mantissa - high, 0.0)))
    choose = selection(held.shape[1], size, lax.axis_index("tp") * share, SHARE_AT, share)
    kept = factor * jnp.dot(held, choose, preferred_element_type=jnp.float32)
    out_ref[:, 4 * rows :, :] = (table + kept).reshape(owners, rows, size)


def project(whole, gain, weights, owners):
    rows = whole.shape[0] * whole.shape[1] // owners
    share = whole.shape[2] // lax.axis_size("tp")
    return pl.pallas_call(
        functools.partial(project_kernel, share),
        out_shape=jax.ShapeDtypeStruct((owners, 5 * rows, weights[0].shape[1]), jnp.float32),
        compiler_params=PARAMS,
        name="project",
    )(whole, gain, *weights)


def load_kernel(ready_ref, state_ref, out_ref, sem):
    copy = pltpu.make_async_copy(state_ref.at[1, :, 0], out_ref, sem)
    copy.start()
    copy.wait()


def load(ready, state):
    _, count, _, size, _ = state.shape
    return pl.pallas_call(
        load_kernel,
        in_specs=[VMEM, HBM],
        out_specs=VMEM,
        out_shape=jax.ShapeDtypeStruct((count, size, size), jnp.float32),
        scratch_shapes=[pltpu.SemaphoreType.DMA],
        compiler_params=WIDE_PARAMS,
        name="load",
    )(ready, state)


def recur(block, made, shift_ref, bound_ref, head_ref, prior_ref, new_ref, loads, stores):
    query, forget_in, value, gate = made
    lower = jax.nn.sigmoid(bound_ref[block : block + 1, :])
    pre = forget_in - shift_ref[block]
    forget = (lower + (1.0 - lower) * jax.nn.sigmoid(pre)).T
    key = ((1.0 - lower) * jax.nn.sigmoid(-pre)).T
    query = query.T
    gate = head_ref[block : block + 1, :] * (gate * jax.nn.sigmoid(gate))
    outs = []
    for n in range(value.shape[0]):
        if loads and n % STEP == 0:
            loads[n // STEP].wait()
        at = slice(n, n + 1)
        updated = forget[:, at] * prior_ref[n] + key[:, at] * value[at, :]
        new_ref[n] = updated
        outs.append(jnp.sum(query[:, at] * updated, axis=0, keepdims=True))
        if n % STEP == STEP - 1:
            stores[n // STEP].start()
    readout = jnp.concatenate(outs, axis=0)
    mean = jnp.mean(readout * readout, axis=1, keepdims=True)
    return (readout * lax.rsqrt(mean + epsilon) * gate).astype(jnp.bfloat16)


def first_kernel(share, parts_ref, shift_ref, bound_ref, head_ref, state_ref, new_ref, own_ref, sent_ref, *scratch):
    prior_s, new_s, in_sems, out_sems = scratch
    loads, stores = [], []
    for n in range(shift_ref.shape[1] // STEP):
        rows = pl.ds(n * STEP, STEP)
        loads.append(pltpu.make_async_copy(state_ref.at[0, rows, 0], prior_s.at[rows], in_sems.at[n]))
        stores.append(pltpu.make_async_copy(new_s.at[rows], new_ref.at[0, rows, 0], out_sems.at[n]))
    for load in loads:
        load.start()
    owners, _, size = parts_ref.shape
    count = shift_ref.shape[1]
    made, squares = [0.0] * 4, 0.0
    for source in range(owners):
        table = parts_ref[source, 4 * count :, :]
        up = jnp.exp2(table[:, 0:1])
        norm = up * 2.0**13
        squares += (table[:, 1:2] + table[:, 2:3]) * norm * norm
        for n in range(4):
            made[n] += parts_ref[source, n * count : (n + 1) * count, :] * up
    scale = lax.rsqrt(squares / D + epsilon)
    made = [scale * total for total in made]
    device = lax.axis_index("dp")
    neighbour = device + 1 - 2 * lax.rem(device, 2)
    for out_ref, holder in ((own_ref, device), (sent_ref, neighbour)):
        kept = 0.0
        for n in range(owners // 2):
            table = parts_ref[near_chunk(n, owners, holder), 4 * count :, :]
            place = selection(size, size, SHARE_AT, n * LANES, share)
            moved = jnp.dot(table.astype(jnp.bfloat16), place, preferred_element_type=jnp.float32)
            kept += jnp.exp2(table[:, 0:1]) * moved
        out_ref[count:, :] = kept.astype(jnp.bfloat16)
    normed = recur(0, made, shift_ref, bound_ref, head_ref, prior_s, new_s, loads, stores)
    own_ref[:count, :] = normed
    sent_ref[:count, :] = normed
    for store in stores:
        store.wait()


def pair_kernel(share, own_ref, came_ref, *refs):
    shards, out_ref = refs[:-1], refs[-1]
    count, size = own_ref.shape[0] // 2, own_ref.shape[1]
    normed = jnp.concatenate([own_ref[:count, :], came_ref[:count, :]], axis=0)
    kept = jnp.concatenate([own_ref[count:, :], came_ref[count:, :]], axis=0)
    width = shards[0].shape[1]
    parts = width // size
    blocks = len(shards) * parts
    for n, shard in enumerate(shards):
        place = selection(size, width, n * LANES, lax.axis_index("tp") * share, share)
        total = jnp.dot(normed, shard[...], preferred_element_type=jnp.float32)
        coded = code(total + jnp.dot(kept, place, preferred_element_type=jnp.float32))
        for part in range(parts):
            for half in range(2):
                block = coded[half * count : (half + 1) * count, part * size : (part + 1) * size]
                out_ref[half * blocks + n * parts + part] = block


def pair_parts(own, came, shards):
    tp, size = lax.axis_size("tp"), own.shape[1]
    return pl.pallas_call(
        functools.partial(pair_kernel, shards[0].shape[1] // tp),
        out_shape=jax.ShapeDtypeStruct((tp, own.shape[0] // 2, size), jnp.float32),
        compiler_params=PARAMS,
        name="pair",
    )(own, came, *shards)


def first(parts, shift, bound, head, share, state):
    _, count, _, size, _ = state.shape
    sides = jax.ShapeDtypeStruct((2 * count, size), jnp.bfloat16)
    return pl.pallas_call(
        functools.partial(first_kernel, share),
        in_specs=[VMEM] * 4 + [HBM],
        out_specs=[HBM, VMEM, VMEM],
        out_shape=[jax.ShapeDtypeStruct(state.shape, jnp.float32), sides, sides],
        scratch_shapes=[pltpu.VMEM((count, size, size), jnp.float32)] * 2
        + [pltpu.SemaphoreType.DMA((count // STEP,))] * 2,
        compiler_params=WIDE_PARAMS,
        name="first",
    )(parts, shift, bound, head, state)


def decoded(parts_ref):
    parts = parts_ref[...]
    return jnp.sum(parts * jnp.abs(parts), axis=0) * 2.0**-12


def next_kernel(parts_ref, out_ref):
    out_ref[...] = jnp.broadcast_to(decoded(parts_ref).astype(jnp.bfloat16), out_ref.shape)


def again_kernel(share, x_ref, *refs):
    shards, (own_ref, sent_ref, kept_ref) = refs[:-3], refs[-3:]
    owners, count, size = kept_ref.shape
    rows = shards[0].shape[0] - PAD
    parts = rows // size
    blocks = len(shards) * parts
    kept_ref[...] = jnp.zeros(kept_ref.shape, kept_ref.dtype)
    at = lax.axis_index("tp") * share
    choose = [selection(rows, size, at, half * share, share) for half in range(2)]
    made, squares = 0.0, 0.0
    for n, shard in enumerate(shards):
        halves = []
        for half in range(2):
            first_block = half * blocks + n * parts
            halves.append(jnp.concatenate([x_ref[first_block + part] for part in range(parts)], axis=1))
        held = jnp.concatenate(halves, axis=0)
        wide = held.astype(jnp.float32)
        squares += jnp.sum(wide * wide, axis=1, keepdims=True)
        gained = (wide * shard[rows : rows + 1, :rows].astype(jnp.float32)).astype(jnp.bfloat16)
        made += jnp.dot(gained, shard[:rows, :], preferred_element_type=jnp.float32)
        kept = [jnp.dot(halves[half], choose[half], preferred_element_type=jnp.float32) for half in range(2)]
        kept_ref[near_chunk(n, owners)] = (kept[0] + kept[1]).astype(kept_ref.dtype)
    for half, out_ref in enumerate((own_ref, sent_ref)):
        row = slice(half * count, (half + 1) * count)
        out_ref[:, : made.shape[1]] = made[row]
        out_ref[:, made.shape[1] :] = jnp.broadcast_to(squares[row], (count, size))


def again(x, shards, owners):
    tp, count, size = x.shape
    rows = shards[0].shape[0] - PAD
    sums = jax.ShapeDtypeStruct((count, shards[0].shape[1] + size), jnp.float32)
    return pl.pallas_call(
        functools.partial(again_kernel, rows // tp),
        out_shape=[sums, sums, jax.ShapeDtypeStruct((owners, count, size), jnp.bfloat16)],
        compiler_params=PARAMS,
        name="again",
    )(x, *shards)


def second_kernel(own_ref, came_ref, shift_ref, bound_ref, head_ref, kept_ref, prior_ref, _, new_ref, out_ref, new_s, sems):
    owners, count, size = kept_ref.shape
    stores = []
    for n in range(count // STEP):
        rows = pl.ds(n * STEP, STEP)
        stores.append(pltpu.make_async_copy(new_s.at[rows], new_ref.at[1, rows, 0], sems.at[n]))
    total = own_ref[...] + came_ref[...]
    scale = lax.rsqrt(total[:, 4 * size : 4 * size + 1] / D + epsilon)
    made = [scale * total[:, n * size : (n + 1) * size] for n in range(4)]
    out_ref[:, count:, :] = kept_ref[...]
    normed = recur(1, made, shift_ref, bound_ref, head_ref, prior_ref, new_s, (), stores)
    out_ref[:, :count, :] = jnp.broadcast_to(normed, (owners, count, size))
    for store in stores:
        store.wait()


def second(own, came, shift, bound, head, kept, prior, target):
    owners, count, size = kept.shape
    return pl.pallas_call(
        second_kernel,
        in_specs=[VMEM] * 7 + [HBM],
        out_specs=[HBM, VMEM],
        out_shape=[
            jax.ShapeDtypeStruct(target.shape, jnp.float32),
            jax.ShapeDtypeStruct((owners, 2 * count, size), jnp.bfloat16),
        ],
        scratch_shapes=[pltpu.VMEM(prior.shape, jnp.float32), pltpu.SemaphoreType.DMA((count // STEP,))],
        input_output_aliases={7: 0},
        compiler_params=SECOND_PARAMS,
        name="second",
    )(own, came, shift, bound, head, kept, prior, target)


def branch_kernel(share, normed_ref, w_ref, out_ref):
    owners, count, size = normed_ref.shape[0], normed_ref.shape[1] // 2, normed_ref.shape[2]
    normed = normed_ref[:, :count, :].reshape(-1, size)
    weight = w_ref[1]
    total = jnp.dot(normed, weight, preferred_element_type=jnp.float32)
    at = lax.axis_index("tp") * share
    mine, other = (selection(size, weight.shape[1], half * share, at, share) for half in range(2))
    flipped = jnp.concatenate([normed_ref[n ^ 1, count:, :] for n in range(owners)], axis=0)
    total += jnp.dot(normed_ref[:, count:, :].reshape(-1, size), mine, preferred_element_type=jnp.float32)
    total += jnp.dot(flipped, other, preferred_element_type=jnp.float32)
    out_ref[...] = code(total).reshape(out_ref.shape)


def branch_parts(normed, weight, owners):
    rows = normed.shape[0] * normed.shape[1] // 2 // owners
    return pl.pallas_call(
        functools.partial(branch_kernel, weight.shape[2] // owners),
        out_shape=jax.ShapeDtypeStruct((owners, rows, weight.shape[2]), jnp.float32),
        compiler_params=PARAMS,
        name="branch",
    )(normed, weight)


def final_kernel(parts_ref, out_ref):
    out_ref[...] = decoded(parts_ref)


def layers(
    tokens,
    state,
    lengths,
    norm_gain,
    w_query,
    w_forget,
    w_input,
    w_gate,
    w_out,
    bound_logit,
    pace,
    head_gain,
):
    tp, dp = lax.axis_size("tp"), lax.axis_size("dp")
    whole = exchange(jnp.broadcast_to(tokens, (tp, *tokens.shape)), "tp")
    weights = (w_query, w_forget, w_input, w_gate)
    gain, *firsts = prep(norm_gain, weights)
    back = near(w_out[0], "dp")
    log_len = jnp.log(lengths.astype(jnp.float32) / LENGTH_MEAN)
    shift = pace[:, None, :] * log_len[None, :, None]

    message = project(whole, gain, firsts, dp).astype(jnp.float16)
    parts = exchange(message, "dp").astype(jnp.float32)
    target, own, sent = first(parts, shift, bound_logit, head_gain, tokens.shape[1] // tp, state)
    packed = pack(1, norm_gain, weights)
    held = near(packed, "dp")
    came = swap(sent, "dp")
    sums = pair_parts(own, came, back)
    parts = exchange_products(sums, "tp")
    copies = pl.pallas_call(
        next_kernel,
        out_shape=jax.ShapeDtypeStruct(parts.shape, jnp.bfloat16),
        compiler_params=PARAMS,
        name="next",
    )(parts)
    joined = exchange(after(copies, held[1:]), "tp")
    prior = load(after(gain, joined), state)
    own, sent, kept = again(joined, held, dp)
    came = swap(sent, "dp")
    target, normed = second(own, came, shift, bound_logit, head_gain, kept, prior, target)
    parts = exchange_products(branch_parts(exchange(normed, "dp"), w_out, tp), "tp")
    result = pl.pallas_call(
        final_kernel,
        out_shape=jax.ShapeDtypeStruct(tokens.shape, jnp.float32),
        compiler_params=PARAMS,
        name="final",
    )(parts)
    return result, target


def solution(mesh):
    in_specs = (
        P(("grp", "tp"), "dp"),
        P(None, ("grp", "dp"), "tp", None, None),
        P(("grp", "dp")),
        P(None, "dp"),
        P(None, "dp", "tp"),
        P(None, "dp", "tp"),
        P(None, "dp", "tp"),
        P(None, "dp", "tp"),
        P(None, "tp", "dp"),
        P(None, "tp"),
        P(None, "tp"),
        P(),
    )
    out_specs = (P(("grp", "tp"), "dp"), P(None, ("grp", "dp"), "tp", None, None))
    return jax.shard_map(layers, mesh=mesh, in_specs=in_specs, out_specs=out_specs, check_vma=False)
```

```python
import functools

import jax
import jax.numpy as jnp
from jax import lax
from jax.experimental import pallas as pl
from jax.experimental.pallas import tpu as pltpu
from jax.sharding import PartitionSpec as P


D = 2048
LENGTH_MEAN = 512
FLOOR = 2.0**-80
PAD = 16
LANES = 32
SHARE_AT = 16
STEP = 8
PARAMS = pltpu.CompilerParams(vmem_limit_bytes=16 << 20)
SECOND_PARAMS = pltpu.CompilerParams(vmem_limit_bytes=50 << 20)
WIDE_PARAMS = pltpu.CompilerParams(vmem_limit_bytes=51 << 20)
PREP_PARAMS = pltpu.CompilerParams(vmem_limit_bytes=54900 << 10)
PACK_PARAMS = pltpu.CompilerParams(vmem_limit_bytes=55300 << 10)
VMEM = pl.BlockSpec(memory_space=pltpu.VMEM)
HBM = pl.BlockSpec(memory_space=pltpu.HBM)

epsilon = 1e-06


def exchange(x, axis):
    return lax.all_to_all(x, axis, split_axis=0, concat_axis=0, tiled=True)


def exchange_products(x, axis):
    return exchange(x.astype(jnp.float16), axis).astype(jnp.float32)


def pack_kernel(block, gain_ref, wq_ref, wf_ref, wi_ref, wg_ref, out_ref, sems):
    rows, size = wq_ref.shape[1:]
    copies = [
        pltpu.make_async_copy(w_ref.at[block], out_ref.at[pl.ds(0, rows), pl.ds(n * size, size)], sems.at[n])
        for n, w_ref in enumerate((wq_ref, wf_ref, wi_ref, wg_ref))
    ]
    for copy in copies:
        copy.start()
    gain = jnp.broadcast_to(gain_ref[block : block + 1, :].astype(jnp.float32), (PAD, rows))
    out_ref[rows:, :rows] = gain.astype(out_ref.dtype)
    out_ref[rows:, rows:] = jnp.zeros((PAD, 4 * size - rows), out_ref.dtype)
    for copy in copies:
        copy.wait()


def pack(block, gain, weights):
    _, rows, size = weights[0].shape
    return pl.pallas_call(
        functools.partial(pack_kernel, block),
        in_specs=[VMEM] + [HBM] * 4,
        out_specs=VMEM,
        out_shape=jax.ShapeDtypeStruct((rows + PAD, 4 * size), jnp.bfloat16),
        scratch_shapes=[pltpu.SemaphoreType.DMA((4,))],
        compiler_params=PACK_PARAMS,
        name="pack",
    )(gain, *weights)


def prep_kernel(gain_ref, *refs):
    weights, row_ref, firsts, sems = refs[:4], refs[4], refs[5:9], refs[9]
    copies = [pltpu.make_async_copy(w_ref.at[0], out, sems.at[n]) for n, (w_ref, out) in enumerate(zip(weights, firsts))]
    for copy in copies:
        copy.start()
    row_ref[...] = gain_ref[0:1, :].astype(jnp.float32)
    for copy in copies:
        copy.wait()


def prep(gain, weights):
    return pl.pallas_call(
        prep_kernel,
        in_specs=[VMEM] + [HBM] * len(weights),
        out_specs=[VMEM] * (1 + len(weights)),
        out_shape=[jax.ShapeDtypeStruct((1, gain.shape[1]), jnp.float32)]
        + [jax.ShapeDtypeStruct(w.shape[1:], w.dtype) for w in weights],
        scratch_shapes=[pltpu.SemaphoreType.DMA((len(weights),))],
        compiler_params=PREP_PARAMS,
        name="prep",
    )(gain, *weights)


def after(x, y):
    return lax.optimization_barrier((x, y))[0]


def side(device):
    return 2 * (device % 2) - 1


def near(shard, axis):
    size = lax.axis_size(axis)
    held = [shard]
    for step in range(1, size // 2):
        pairs = [((n + side(n) * step) % size, n) for n in range(size)]
        held.append(lax.ppermute(shard, axis, pairs))
    return held


def swap(x, axis):
    return lax.ppermute(x, axis, [(n, n ^ 1) for n in range(lax.axis_size(axis))])


def near_chunk(n, owners, device=None):
    device = lax.axis_index("dp") if device is None else device
    return lax.rem(device + (2 * lax.rem(device, 2) - 1) * n + owners, owners)


def selection(rows, columns, start_row, start_column, share):
    row = lax.broadcasted_iota(jnp.int32, (rows, columns), 0) - start_row
    column = lax.broadcasted_iota(jnp.int32, (rows, columns), 1) - start_column
    inside = (row >= 0) & (row < share) & (row == column)
    return jnp.where(inside, 1.0, 0.0).astype(jnp.bfloat16)


def code(total):
    root = jnp.sqrt(jnp.abs(total)) * 2.0**6
    return jnp.where(total < 0.0, -root, root)


def scaled(squares, bits):
    power = jnp.ceil(0.5 * jnp.log2(jnp.maximum(squares, FLOOR)))
    down = jnp.exp2(-power)
    mantissa = squares * down * down
    high = mantissa.astype(jnp.bfloat16).astype(jnp.float32)
    return down * 2.0**bits, (power - bits, high, mantissa - high)


def project_kernel(share, x_ref, gain_ref, wq_ref, wf_ref, wi_ref, wg_ref, out_ref):
    owners, size = out_ref.shape[0], out_ref.shape[-1]
    rows = out_ref.shape[1] // 5
    held = x_ref[...].reshape(owners * rows, x_ref.shape[-1])
    x = held.astype(jnp.float32)
    squares = jnp.sum(x * x, axis=1, keepdims=True)
    power = jnp.ceil(0.5 * jnp.log2(jnp.maximum(squares, FLOOR)))
    down = jnp.exp2(-power)
    factor = down * 2.0**13
    gained = (x * gain_ref[...]).astype(jnp.bfloat16)
    for n, w_ref in enumerate((wq_ref, wf_ref, wi_ref, wg_ref)):
        partial = factor * jnp.dot(gained, w_ref[...], preferred_element_type=jnp.float32)
        out_ref[:, n * rows : (n + 1) * rows, :] = partial.reshape(owners, rows, size)
    mantissa = squares * down * down
    high = mantissa.astype(jnp.bfloat16).astype(jnp.float32)
    lane = lax.broadcasted_iota(jnp.int32, (owners * rows, size), 1)
    table = jnp.where(lane == 0, power - 13.0, jnp.where(lane == 1, high, jnp.where(lane == 2, mantissa - high, 0.0)))
    choose = selection(held.shape[1], size, lax.axis_index("tp") * share, SHARE_AT, share)
    kept = factor * jnp.dot(held, choose, preferred_element_type=jnp.float32)
    out_ref[:, 4 * rows :, :] = (table + kept).reshape(owners, rows, size)


def project(whole, gain, weights, owners):
    rows = whole.shape[0] * whole.shape[1] // owners
    share = whole.shape[2] // lax.axis_size("tp")
    return pl.pallas_call(
        functools.partial(project_kernel, share),
        out_shape=jax.ShapeDtypeStruct((owners, 5 * rows, weights[0].shape[1]), jnp.float32),
        compiler_params=PARAMS,
        name="project",
    )(whole, gain, *weights)


def load_kernel(ready_ref, state_ref, out_ref, sem):
    copy = pltpu.make_async_copy(state_ref.at[1, :, 0], out_ref, sem)
    copy.start()
    copy.wait()


def load(ready, state):
    _, count, _, size, _ = state.shape
    return pl.pallas_call(
        load_kernel,
        in_specs=[VMEM, HBM],
        out_specs=VMEM,
        out_shape=jax.ShapeDtypeStruct((count, size, size), jnp.float32),
        scratch_shapes=[pltpu.SemaphoreType.DMA],
        compiler_params=WIDE_PARAMS,
        name="load",
    )(ready, state)


def recur(block, made, shift_ref, bound_ref, head_ref, prior_ref, new_ref, loads, stores):
    query, forget_in, value, gate = made
    lower = jax.nn.sigmoid(bound_ref[block : block + 1, :])
    pre = forget_in - shift_ref[block]
    forget = (lower + (1.0 - lower) * jax.nn.sigmoid(pre)).T
    key = ((1.0 - lower) * jax.nn.sigmoid(-pre)).T
    query = query.T
    gate = head_ref[block : block + 1, :] * (gate * jax.nn.sigmoid(gate))
    outs = []
    for n in range(value.shape[0]):
        if loads and n % STEP == 0:
            loads[n // STEP].wait()
        at = slice(n, n + 1)
        updated = forget[:, at] * prior_ref[n] + key[:, at] * value[at, :]
        new_ref[n] = updated
        outs.append(jnp.sum(query[:, at] * updated, axis=0, keepdims=True))
        if n % STEP == STEP - 1:
            stores[n // STEP].start()
    readout = jnp.concatenate(outs, axis=0)
    mean = jnp.mean(readout * readout, axis=1, keepdims=True)
    return (readout * lax.rsqrt(mean + epsilon) * gate).astype(jnp.bfloat16)


def first_kernel(share, parts_ref, shift_ref, bound_ref, head_ref, state_ref, new_ref, own_ref, sent_ref, *scratch):
    prior_s, new_s, in_sems, out_sems = scratch
    loads, stores = [], []
    for n in range(shift_ref.shape[1] // STEP):
        rows = pl.ds(n * STEP, STEP)
        loads.append(pltpu.make_async_copy(state_ref.at[0, rows, 0], prior_s.at[rows], in_sems.at[n]))
        stores.append(pltpu.make_async_copy(new_s.at[rows], new_ref.at[0, rows, 0], out_sems.at[n]))
    for load in loads:
        load.start()
    owners, _, size = parts_ref.shape
    count = shift_ref.shape[1]
    made, squares = [0.0] * 4, 0.0
    for source in range(owners):
        table = parts_ref[source, 4 * count :, :]
        up = jnp.exp2(table[:, 0:1])
        norm = up * 2.0**13
        squares += (table[:, 1:2] + table[:, 2:3]) * norm * norm
        for n in range(4):
            made[n] += parts_ref[source, n * count : (n + 1) * count, :] * up
    scale = lax.rsqrt(squares / D + epsilon)
    made = [scale * total for total in made]
    device = lax.axis_index("dp")
    neighbour = device + 1 - 2 * lax.rem(device, 2)
    for out_ref, holder in ((own_ref, device), (sent_ref, neighbour)):
        kept = 0.0
        for n in range(owners // 2):
            table = parts_ref[near_chunk(n, owners, holder), 4 * count :, :]
            place = selection(size, size, SHARE_AT, n * LANES, share)
            moved = jnp.dot(table.astype(jnp.bfloat16), place, preferred_element_type=jnp.float32)
            kept += jnp.exp2(table[:, 0:1]) * moved
        out_ref[count:, :] = kept.astype(jnp.bfloat16)
    normed = recur(0, made, shift_ref, bound_ref, head_ref, prior_s, new_s, loads, stores)
    own_ref[:count, :] = normed
    sent_ref[:count, :] = normed
    for store in stores:
        store.wait()


def pair_kernel(share, own_ref, came_ref, *refs):
    shards, out_ref = refs[:-1], refs[-1]
    count, size = own_ref.shape[0] // 2, own_ref.shape[1]
    normed = jnp.concatenate([own_ref[:count, :], came_ref[:count, :]], axis=0)
    kept = jnp.concatenate([own_ref[count:, :], came_ref[count:, :]], axis=0)
    width = shards[0].shape[1]
    parts = width // size
    blocks = len(shards) * parts
    for n, shard in enumerate(shards):
        place = selection(size, width, n * LANES, lax.axis_index("tp") * share, share)
        total = jnp.dot(normed, shard[...], preferred_element_type=jnp.float32)
        coded = code(total + jnp.dot(kept, place, preferred_element_type=jnp.float32))
        for part in range(parts):
            for half in range(2):
                block = coded[half * count : (half + 1) * count, part * size : (part + 1) * size]
                out_ref[half * blocks + n * parts + part] = block


def pair_parts(own, came, shards):
    tp, size = lax.axis_size("tp"), own.shape[1]
    return pl.pallas_call(
        functools.partial(pair_kernel, shards[0].shape[1] // tp),
        out_shape=jax.ShapeDtypeStruct((tp, own.shape[0] // 2, size), jnp.float32),
        compiler_params=PARAMS,
        name="pair",
    )(own, came, *shards)


def first(parts, shift, bound, head, share, state):
    _, count, _, size, _ = state.shape
    sides = jax.ShapeDtypeStruct((2 * count, size), jnp.bfloat16)
    return pl.pallas_call(
        functools.partial(first_kernel, share),
        in_specs=[VMEM] * 4 + [HBM],
        out_specs=[HBM, VMEM, VMEM],
        out_shape=[jax.ShapeDtypeStruct(state.shape, jnp.float32), sides, sides],
        scratch_shapes=[pltpu.VMEM((count, size, size), jnp.float32)] * 2
        + [pltpu.SemaphoreType.DMA((count // STEP,))] * 2,
        compiler_params=WIDE_PARAMS,
        name="first",
    )(parts, shift, bound, head, state)


def decoded(parts_ref):
    parts = parts_ref[...]
    return jnp.sum(parts * jnp.abs(parts), axis=0) * 2.0**-12


def next_kernel(parts_ref, out_ref):
    out_ref[...] = jnp.broadcast_to(decoded(parts_ref).astype(jnp.bfloat16), out_ref.shape)


def again_kernel(share, x_ref, *refs):
    shards, (own_ref, sent_ref, kept_ref) = refs[:-3], refs[-3:]
    owners, packed, size = kept_ref.shape
    count = x_ref.shape[1]
    rows = shards[0].shape[0] - PAD
    parts = rows // size
    blocks = len(shards) * parts
    kept_ref[...] = jnp.zeros(kept_ref.shape, kept_ref.dtype)
    at = lax.axis_index("tp") * share
    choose = [selection(rows, size, at, half * share, share) for half in range(2)]
    made, squares = 0.0, 0.0
    for n, shard in enumerate(shards):
        halves = []
        for half in range(2):
            first_block = half * blocks + n * parts
            halves.append(jnp.concatenate([x_ref[first_block + part] for part in range(parts)], axis=1))
        held = jnp.concatenate(halves, axis=0)
        wide = held.astype(jnp.float32)
        squares += jnp.sum(wide * wide, axis=1, keepdims=True)
        gained = (wide * shard[rows : rows + 1, :rows].astype(jnp.float32)).astype(jnp.bfloat16)
        made += jnp.dot(gained, shard[:rows, :], preferred_element_type=jnp.float32)
        kept = [jnp.dot(halves[half], choose[half], preferred_element_type=jnp.float32) for half in range(2)]
        kept = kept[0] + kept[1]
        block = kept[:packed]
        for group in range(1, count // packed):
            block += pltpu.roll(kept[group * packed : (group + 1) * packed], group * LANES, 1)
        kept_ref[near_chunk(n, owners)] = block.astype(kept_ref.dtype)
    own_ref[:, : made.shape[1]] = made[:count]
    own_ref[:, made.shape[1] :] = jnp.broadcast_to(squares[:count], (count, size))
    factor, columns = scaled(squares[count:], 12)
    sent_ref[:, : made.shape[1]] = factor * made[count:]
    lane = lax.broadcasted_iota(jnp.int32, (count, size), 1)
    table = jnp.where(lane == 0, columns[0], jnp.where(lane == 1, columns[1], jnp.where(lane == 2, columns[2], 0.0)))
    sent_ref[:, made.shape[1] :] = table


def again(x, shards, owners):
    tp, count, size = x.shape
    rows = shards[0].shape[0] - PAD
    sums = jax.ShapeDtypeStruct((count, shards[0].shape[1] + size), jnp.float32)
    return pl.pallas_call(
        functools.partial(again_kernel, rows // tp),
        out_shape=[sums, sums, jax.ShapeDtypeStruct((owners, count * LANES // size, size), jnp.bfloat16)],
        compiler_params=PARAMS,
        name="again",
    )(x, *shards)


def second_kernel(own_ref, came_ref, shift_ref, bound_ref, head_ref, kept_ref, prior_ref, _, new_ref, out_ref, new_s, sems):
    owners, _, size = kept_ref.shape
    count = shift_ref.shape[1]
    stores = []
    for n in range(count // STEP):
        rows = pl.ds(n * STEP, STEP)
        stores.append(pltpu.make_async_copy(new_s.at[rows], new_ref.at[1, rows, 0], sems.at[n]))
    table = came_ref[:, 4 * size :]
    up = jnp.exp2(table[:, 0:1])
    norm = up * 2.0**12
    squares = own_ref[:, 4 * size : 4 * size + 1] + (table[:, 1:2] + table[:, 2:3]) * norm * norm
    scale = lax.rsqrt(squares / D + epsilon)
    lanes = [slice(n * size, (n + 1) * size) for n in range(4)]
    made = [scale * (own_ref[:, lane] + up * came_ref[:, lane]) for lane in lanes]
    out_ref[:, count:, :] = kept_ref[...]
    normed = recur(1, made, shift_ref, bound_ref, head_ref, prior_ref, new_s, (), stores)
    out_ref[:, :count, :] = jnp.broadcast_to(normed, (owners, count, size))
    for store in stores:
        store.wait()


def second(own, came, shift, bound, head, kept, prior, target):
    owners, packed, size = kept.shape
    count = prior.shape[0]
    return pl.pallas_call(
        second_kernel,
        in_specs=[VMEM] * 7 + [HBM],
        out_specs=[HBM, VMEM],
        out_shape=[
            jax.ShapeDtypeStruct(target.shape, jnp.float32),
            jax.ShapeDtypeStruct((owners, count + packed, size), jnp.bfloat16),
        ],
        scratch_shapes=[pltpu.VMEM(prior.shape, jnp.float32), pltpu.SemaphoreType.DMA((count // STEP,))],
        input_output_aliases={7: 0},
        compiler_params=SECOND_PARAMS,
        name="second",
    )(own, came, shift, bound, head, kept, prior, target)


def branch_kernel(share, count, normed_ref, w_ref, out_ref):
    owners, both, size = normed_ref.shape
    packed = both - count
    normed = normed_ref[:, :count, :].reshape(-1, size)
    weight = w_ref[1]
    total = jnp.dot(normed, weight, preferred_element_type=jnp.float32)
    at = lax.axis_index("tp") * share
    held = [normed_ref[:, count:, :].reshape(-1, size)]
    held.append(jnp.concatenate([normed_ref[n ^ 1, count:, :] for n in range(owners)], axis=0))
    groups = []
    for group in range(count // packed):
        kept = 0.0
        for half in range(2):
            place = selection(size, weight.shape[1], group * LANES + half * share, at, share)
            kept += jnp.dot(held[half], place, preferred_element_type=jnp.float32)
        groups.append(kept)
    rows = [groups[g][n * packed : (n + 1) * packed] for n in range(owners) for g in range(len(groups))]
    out_ref[...] = code(total + jnp.concatenate(rows, axis=0)).reshape(out_ref.shape)


def branch_parts(normed, weight, owners, count):
    return pl.pallas_call(
        functools.partial(branch_kernel, weight.shape[2] // owners, count),
        out_shape=jax.ShapeDtypeStruct((owners, normed.shape[0] * count // owners, weight.shape[2]), jnp.float32),
        compiler_params=PARAMS,
        name="branch",
    )(normed, weight)


def final_kernel(parts_ref, out_ref):
    out_ref[...] = decoded(parts_ref)


def layers(
    tokens,
    state,
    lengths,
    norm_gain,
    w_query,
    w_forget,
    w_input,
    w_gate,
    w_out,
    bound_logit,
    pace,
    head_gain,
):
    tp, dp = lax.axis_size("tp"), lax.axis_size("dp")
    whole = exchange(jnp.broadcast_to(tokens, (tp, *tokens.shape)), "tp")
    weights = (w_query, w_forget, w_input, w_gate)
    gain, *firsts = prep(norm_gain, weights)
    back = near(w_out[0], "dp")
    log_len = jnp.log(lengths.astype(jnp.float32) / LENGTH_MEAN)
    shift = pace[:, None, :] * log_len[None, :, None]

    message = project(whole, gain, firsts, dp).astype(jnp.float16)
    parts = exchange(message, "dp").astype(jnp.float32)
    target, own, sent = first(parts, shift, bound_logit, head_gain, tokens.shape[1] // tp, state)
    packed = pack(1, norm_gain, weights)
    held = near(packed, "dp")
    came = swap(sent, "dp")
    sums = pair_parts(own, came, back)
    parts = exchange_products(sums, "tp")
    copies = pl.pallas_call(
        next_kernel,
        out_shape=jax.ShapeDtypeStruct(parts.shape, jnp.bfloat16),
        compiler_params=PARAMS,
        name="next",
    )(parts)
    joined = exchange(after(copies, held[1:]), "tp")
    prior = load(after(gain, joined), state)
    own, sent, kept = again(joined, held, dp)
    came = swap(sent.astype(jnp.float16), "dp").astype(jnp.float32)
    target, normed = second(own, came, shift, bound_logit, head_gain, kept, prior, target)
    parts = exchange_products(branch_parts(exchange(normed, "dp"), w_out, tp, lengths.shape[0]), "tp")
    result = pl.pallas_call(
        final_kernel,
        out_shape=jax.ShapeDtypeStruct(tokens.shape, jnp.float32),
        compiler_params=PARAMS,
        name="final",
    )(parts)
    return result, target


def solution(mesh):
    in_specs = (
        P(("grp", "tp"), "dp"),
        P(None, ("grp", "dp"), "tp", None, None),
        P(("grp", "dp")),
        P(None, "dp"),
        P(None, "dp", "tp"),
        P(None, "dp", "tp"),
        P(None, "dp", "tp"),
        P(None, "dp", "tp"),
        P(None, "tp", "dp"),
        P(None, "tp"),
        P(None, "tp"),
        P(),
    )
    out_specs = (P(("grp", "tp"), "dp"), P(None, ("grp", "dp"), "tp", None, None))
    return jax.shard_map(layers, mesh=mesh, in_specs=in_specs, out_specs=out_specs, check_vma=False)
```

```python
import functools

import jax
import jax.numpy as jnp
from jax import lax
from jax.experimental import pallas as pl
from jax.experimental.pallas import tpu as pltpu
from jax.sharding import PartitionSpec as P


D = 2048
LENGTH_MEAN = 512
FLOOR = 2.0**-80
PAD = 16
LANES = 32
SHARE_AT = 16
STEP = 8
PARAMS = pltpu.CompilerParams(vmem_limit_bytes=16 << 20)
SECOND_PARAMS = pltpu.CompilerParams(vmem_limit_bytes=50 << 20)
WIDE_PARAMS = pltpu.CompilerParams(vmem_limit_bytes=51 << 20)
PREP_PARAMS = pltpu.CompilerParams(vmem_limit_bytes=54900 << 10)
PACK_PARAMS = pltpu.CompilerParams(vmem_limit_bytes=55300 << 10)
VMEM = pl.BlockSpec(memory_space=pltpu.VMEM)
HBM = pl.BlockSpec(memory_space=pltpu.HBM)

epsilon = 1e-06


def exchange(x, axis):
    return lax.all_to_all(x, axis, split_axis=0, concat_axis=0, tiled=True)


def exchange_products(x, axis):
    return exchange(x.astype(jnp.float16), axis).astype(jnp.float32)


def pack_kernel(block, gain_ref, wq_ref, wf_ref, wi_ref, wg_ref, out_ref, sems):
    rows, size = wq_ref.shape[1:]
    copies = [
        pltpu.make_async_copy(w_ref.at[block], out_ref.at[pl.ds(0, rows), pl.ds(n * size, size)], sems.at[n])
        for n, w_ref in enumerate((wq_ref, wf_ref, wi_ref, wg_ref))
    ]
    for copy in copies:
        copy.start()
    gain = jnp.broadcast_to(gain_ref[block : block + 1, :].astype(jnp.float32), (PAD, rows))
    out_ref[rows:, :rows] = gain.astype(out_ref.dtype)
    out_ref[rows:, rows:] = jnp.zeros((PAD, 4 * size - rows), out_ref.dtype)
    for copy in copies:
        copy.wait()


def pack(block, gain, weights):
    _, rows, size = weights[0].shape
    return pl.pallas_call(
        functools.partial(pack_kernel, block),
        in_specs=[VMEM] + [HBM] * 4,
        out_specs=VMEM,
        out_shape=jax.ShapeDtypeStruct((rows + PAD, 4 * size), jnp.bfloat16),
        scratch_shapes=[pltpu.SemaphoreType.DMA((4,))],
        compiler_params=PACK_PARAMS,
        name="pack",
    )(gain, *weights)


def prep_kernel(gain_ref, *refs):
    weights, row_ref, firsts, sems = refs[:4], refs[4], refs[5:9], refs[9]
    copies = [pltpu.make_async_copy(w_ref.at[0], out, sems.at[n]) for n, (w_ref, out) in enumerate(zip(weights, firsts))]
    for copy in copies:
        copy.start()
    row_ref[...] = gain_ref[0:1, :].astype(jnp.float32)
    for copy in copies:
        copy.wait()


def prep(gain, weights):
    return pl.pallas_call(
        prep_kernel,
        in_specs=[VMEM] + [HBM] * len(weights),
        out_specs=[VMEM] * (1 + len(weights)),
        out_shape=[jax.ShapeDtypeStruct((1, gain.shape[1]), jnp.float32)]
        + [jax.ShapeDtypeStruct(w.shape[1:], w.dtype) for w in weights],
        scratch_shapes=[pltpu.SemaphoreType.DMA((len(weights),))],
        compiler_params=PREP_PARAMS,
        name="prep",
    )(gain, *weights)


def after(x, y):
    return lax.optimization_barrier((x, y))[0]


def side(device):
    return 2 * (device % 2) - 1


def near(shard, axis):
    size = lax.axis_size(axis)
    held = [shard]
    for step in range(1, size // 2):
        pairs = [((n + side(n) * step) % size, n) for n in range(size)]
        held.append(lax.ppermute(shard, axis, pairs))
    return held


def swap(x, axis):
    return lax.ppermute(x, axis, [(n, n ^ 1) for n in range(lax.axis_size(axis))])


def near_chunk(n, owners, device=None):
    device = lax.axis_index("dp") if device is None else device
    return lax.rem(device + (2 * lax.rem(device, 2) - 1) * n + owners, owners)


def selection(rows, columns, start_row, start_column, share):
    row = lax.broadcasted_iota(jnp.int32, (rows, columns), 0) - start_row
    column = lax.broadcasted_iota(jnp.int32, (rows, columns), 1) - start_column
    inside = (row >= 0) & (row < share) & (row == column)
    return jnp.where(inside, 1.0, 0.0).astype(jnp.bfloat16)


def code(total):
    root = jnp.sqrt(jnp.abs(total)) * 2.0**6
    return jnp.where(total < 0.0, -root, root)


def packed_rows(block):
    size = block.shape[1]
    count = block.shape[0] * LANES // size
    total = block[:count]
    for group in range(1, size // LANES):
        total += pltpu.roll(block[group * count : (group + 1) * count], group * LANES, 1)
    return total


def unpacked_rows(block):
    size = block.shape[1]
    groups = [block] + [pltpu.roll(block, size - group * LANES, 1) for group in range(1, size // LANES)]
    return jnp.concatenate(groups, axis=0)


def scaled(squares, bits):
    power = jnp.ceil(0.5 * jnp.log2(jnp.maximum(squares, FLOOR)))
    down = jnp.exp2(-power)
    mantissa = squares * down * down
    high = mantissa.astype(jnp.bfloat16).astype(jnp.float32)
    return down * 2.0**bits, (power - bits, high, mantissa - high)


def project_kernel(share, x_ref, gain_ref, wq_ref, wf_ref, wi_ref, wg_ref, out_ref):
    owners, size = out_ref.shape[0], out_ref.shape[-1]
    rows = x_ref.shape[0] * x_ref.shape[1] // owners
    held = x_ref[...].reshape(owners * rows, x_ref.shape[-1])
    x = held.astype(jnp.float32)
    squares = jnp.sum(x * x, axis=1, keepdims=True)
    power = jnp.ceil(0.5 * jnp.log2(jnp.maximum(squares, FLOOR)))
    down = jnp.exp2(-power)
    factor = down * 2.0**13
    gained = (x * gain_ref[...]).astype(jnp.bfloat16)
    for n, w_ref in enumerate((wq_ref, wf_ref, wi_ref, wg_ref)):
        partial = factor * jnp.dot(gained, w_ref[...], preferred_element_type=jnp.float32)
        out_ref[:, n * rows : (n + 1) * rows, :] = partial.reshape(owners, rows, size)
    mantissa = squares * down * down
    high = mantissa.astype(jnp.bfloat16).astype(jnp.float32)
    lane = lax.broadcasted_iota(jnp.int32, (owners * rows, size), 1)
    table = jnp.where(lane == 0, power - 13.0, jnp.where(lane == 1, high, jnp.where(lane == 2, mantissa - high, 0.0)))
    choose = selection(held.shape[1], size, lax.axis_index("tp") * share, SHARE_AT, share)
    kept = factor * jnp.dot(held, choose, preferred_element_type=jnp.float32)
    both = table + kept
    for owner in range(owners):
        out_ref[owner, 4 * rows :, :] = packed_rows(both[owner * rows : (owner + 1) * rows])


def project(whole, gain, weights, owners):
    rows = whole.shape[0] * whole.shape[1] // owners
    share = whole.shape[2] // lax.axis_size("tp")
    extra = rows * LANES // weights[0].shape[1]
    return pl.pallas_call(
        functools.partial(project_kernel, share),
        out_shape=jax.ShapeDtypeStruct((owners, 4 * rows + extra, weights[0].shape[1]), jnp.float32),
        compiler_params=PARAMS,
        name="project",
    )(whole, gain, *weights)


def load_kernel(ready_ref, state_ref, out_ref, sem):
    copy = pltpu.make_async_copy(state_ref.at[1, :, 0], out_ref, sem)
    copy.start()
    copy.wait()


def load(ready, state):
    _, count, _, size, _ = state.shape
    return pl.pallas_call(
        load_kernel,
        in_specs=[VMEM, HBM],
        out_specs=VMEM,
        out_shape=jax.ShapeDtypeStruct((count, size, size), jnp.float32),
        scratch_shapes=[pltpu.SemaphoreType.DMA],
        compiler_params=WIDE_PARAMS,
        name="load",
    )(ready, state)


def recur(block, made, shift_ref, bound_ref, head_ref, prior_ref, new_ref, loads, stores):
    query, forget_in, value, gate = made
    lower = jax.nn.sigmoid(bound_ref[block : block + 1, :])
    pre = forget_in - shift_ref[block]
    forget = (lower + (1.0 - lower) * jax.nn.sigmoid(pre)).T
    key = ((1.0 - lower) * jax.nn.sigmoid(-pre)).T
    query = query.T
    gate = head_ref[block : block + 1, :] * (gate * jax.nn.sigmoid(gate))
    outs = []
    for n in range(value.shape[0]):
        if loads and n % STEP == 0:
            loads[n // STEP].wait()
        at = slice(n, n + 1)
        updated = forget[:, at] * prior_ref[n] + key[:, at] * value[at, :]
        new_ref[n] = updated
        outs.append(jnp.sum(query[:, at] * updated, axis=0, keepdims=True))
        if n % STEP == STEP - 1:
            stores[n // STEP].start()
    readout = jnp.concatenate(outs, axis=0)
    mean = jnp.mean(readout * readout, axis=1, keepdims=True)
    return (readout * lax.rsqrt(mean + epsilon) * gate).astype(jnp.bfloat16)


def first_kernel(share, parts_ref, shift_ref, bound_ref, head_ref, state_ref, new_ref, own_ref, sent_ref, *scratch):
    prior_s, new_s, in_sems, out_sems = scratch
    loads, stores = [], []
    for n in range(shift_ref.shape[1] // STEP):
        rows = pl.ds(n * STEP, STEP)
        loads.append(pltpu.make_async_copy(state_ref.at[0, rows, 0], prior_s.at[rows], in_sems.at[n]))
        stores.append(pltpu.make_async_copy(new_s.at[rows], new_ref.at[0, rows, 0], out_sems.at[n]))
    for load in loads:
        load.start()
    owners, _, size = parts_ref.shape
    count = shift_ref.shape[1]
    made, squares = [0.0] * 4, 0.0
    for source in range(owners):
        table = unpacked_rows(parts_ref[source, 4 * count :, :])
        up = jnp.exp2(table[:, 0:1])
        norm = up * 2.0**13
        squares += (table[:, 1:2] + table[:, 2:3]) * norm * norm
        for n in range(4):
            made[n] += parts_ref[source, n * count : (n + 1) * count, :] * up
    scale = lax.rsqrt(squares / D + epsilon)
    made = [scale * total for total in made]
    device = lax.axis_index("dp")
    neighbour = device + 1 - 2 * lax.rem(device, 2)
    for out_ref, holder in ((own_ref, device), (sent_ref, neighbour)):
        kept = 0.0
        for n in range(owners // 2):
            table = unpacked_rows(parts_ref[near_chunk(n, owners, holder), 4 * count :, :])
            place = selection(size, size, SHARE_AT, n * LANES, share)
            moved = jnp.dot(table.astype(jnp.bfloat16), place, preferred_element_type=jnp.float32)
            kept += jnp.exp2(table[:, 0:1]) * moved
        out_ref[count:, :] = kept.astype(jnp.bfloat16)
    normed = recur(0, made, shift_ref, bound_ref, head_ref, prior_s, new_s, loads, stores)
    own_ref[:count, :] = normed
    sent_ref[:count, :] = normed
    for store in stores:
        store.wait()


def pair_kernel(share, own_ref, came_ref, *refs):
    shards, out_ref = refs[:-1], refs[-1]
    count, size = own_ref.shape[0] // 2, own_ref.shape[1]
    normed = jnp.concatenate([own_ref[:count, :], came_ref[:count, :]], axis=0)
    kept = jnp.concatenate([own_ref[count:, :], came_ref[count:, :]], axis=0)
    width = shards[0].shape[1]
    parts = width // size
    blocks = len(shards) * parts
    for n, shard in enumerate(shards):
        place = selection(size, width, n * LANES, lax.axis_index("tp") * share, share)
        total = jnp.dot(normed, shard[...], preferred_element_type=jnp.float32)
        coded = code(total + jnp.dot(kept, place, preferred_element_type=jnp.float32))
        for part in range(parts):
            for half in range(2):
                block = coded[half * count : (half + 1) * count, part * size : (part + 1) * size]
                out_ref[half * blocks + n * parts + part] = block


def pair_parts(own, came, shards):
    tp, size = lax.axis_size("tp"), own.shape[1]
    return pl.pallas_call(
        functools.partial(pair_kernel, shards[0].shape[1] // tp),
        out_shape=jax.ShapeDtypeStruct((tp, own.shape[0] // 2, size), jnp.float32),
        compiler_params=PARAMS,
        name="pair",
    )(own, came, *shards)


def first(parts, shift, bound, head, share, state):
    _, count, _, size, _ = state.shape
    sides = jax.ShapeDtypeStruct((2 * count, size), jnp.bfloat16)
    return pl.pallas_call(
        functools.partial(first_kernel, share),
        in_specs=[VMEM] * 4 + [HBM],
        out_specs=[HBM, VMEM, VMEM],
        out_shape=[jax.ShapeDtypeStruct(state.shape, jnp.float32), sides, sides],
        scratch_shapes=[pltpu.VMEM((count, size, size), jnp.float32)] * 2
        + [pltpu.SemaphoreType.DMA((count // STEP,))] * 2,
        compiler_params=WIDE_PARAMS,
        name="first",
    )(parts, shift, bound, head, state)


def decoded(parts_ref):
    parts = parts_ref[...]
    return jnp.sum(parts * jnp.abs(parts), axis=0) * 2.0**-12


def next_kernel(parts_ref, out_ref):
    out_ref[...] = jnp.broadcast_to(decoded(parts_ref).astype(jnp.bfloat16), out_ref.shape)


def again_kernel(share, x_ref, *refs):
    shards, (own_ref, sent_ref, kept_ref) = refs[:-3], refs[-3:]
    owners, _, size = kept_ref.shape
    count = x_ref.shape[1]
    rows = shards[0].shape[0] - PAD
    parts = rows // size
    blocks = len(shards) * parts
    kept_ref[...] = jnp.zeros(kept_ref.shape, kept_ref.dtype)
    at = lax.axis_index("tp") * share
    choose = [selection(rows, size, at, half * share, share) for half in range(2)]
    made, squares = 0.0, 0.0
    for n, shard in enumerate(shards):
        halves = []
        for half in range(2):
            first_block = half * blocks + n * parts
            halves.append(jnp.concatenate([x_ref[first_block + part] for part in range(parts)], axis=1))
        held = jnp.concatenate(halves, axis=0)
        wide = held.astype(jnp.float32)
        squares += jnp.sum(wide * wide, axis=1, keepdims=True)
        gained = (wide * shard[rows : rows + 1, :rows].astype(jnp.float32)).astype(jnp.bfloat16)
        made += jnp.dot(gained, shard[:rows, :], preferred_element_type=jnp.float32)
        kept = [jnp.dot(halves[half], choose[half], preferred_element_type=jnp.float32) for half in range(2)]
        kept = kept[0] + kept[1]
        kept_ref[near_chunk(n, owners)] = packed_rows(kept).astype(kept_ref.dtype)
    own_ref[:, : made.shape[1]] = made[:count]
    own_ref[:, made.shape[1] :] = jnp.broadcast_to(squares[:count], (count, size))
    factor, columns = scaled(squares[count:], 12)
    sent_ref[:, : made.shape[1]] = factor * made[count:]
    lane = lax.broadcasted_iota(jnp.int32, (count, size), 1)
    table = jnp.where(lane == 0, columns[0], jnp.where(lane == 1, columns[1], jnp.where(lane == 2, columns[2], 0.0)))
    sent_ref[:, made.shape[1] :] = table


def again(x, shards, owners):
    tp, count, size = x.shape
    rows = shards[0].shape[0] - PAD
    sums = jax.ShapeDtypeStruct((count, shards[0].shape[1] + size), jnp.float32)
    return pl.pallas_call(
        functools.partial(again_kernel, rows // tp),
        out_shape=[sums, sums, jax.ShapeDtypeStruct((owners, count * LANES // size, size), jnp.bfloat16)],
        compiler_params=PARAMS,
        name="again",
    )(x, *shards)


def second_kernel(own_ref, came_ref, shift_ref, bound_ref, head_ref, kept_ref, prior_ref, _, new_ref, out_ref, new_s, sems):
    owners, _, size = kept_ref.shape
    count = shift_ref.shape[1]
    stores = []
    for n in range(count // STEP):
        rows = pl.ds(n * STEP, STEP)
        stores.append(pltpu.make_async_copy(new_s.at[rows], new_ref.at[1, rows, 0], sems.at[n]))
    table = came_ref[:, 4 * size :]
    up = jnp.exp2(table[:, 0:1])
    norm = up * 2.0**12
    squares = own_ref[:, 4 * size : 4 * size + 1] + (table[:, 1:2] + table[:, 2:3]) * norm * norm
    scale = lax.rsqrt(squares / D + epsilon)
    lanes = [slice(n * size, (n + 1) * size) for n in range(4)]
    made = [scale * (own_ref[:, lane] + up * came_ref[:, lane]) for lane in lanes]
    out_ref[:, count:, :] = kept_ref[...]
    normed = recur(1, made, shift_ref, bound_ref, head_ref, prior_ref, new_s, (), stores)
    out_ref[:, :count, :] = jnp.broadcast_to(normed, (owners, count, size))
    for store in stores:
        store.wait()


def second(own, came, shift, bound, head, kept, prior, target):
    owners, packed, size = kept.shape
    count = prior.shape[0]
    return pl.pallas_call(
        second_kernel,
        in_specs=[VMEM] * 7 + [HBM],
        out_specs=[HBM, VMEM],
        out_shape=[
            jax.ShapeDtypeStruct(target.shape, jnp.float32),
            jax.ShapeDtypeStruct((owners, count + packed, size), jnp.bfloat16),
        ],
        scratch_shapes=[pltpu.VMEM(prior.shape, jnp.float32), pltpu.SemaphoreType.DMA((count // STEP,))],
        input_output_aliases={7: 0},
        compiler_params=SECOND_PARAMS,
        name="second",
    )(own, came, shift, bound, head, kept, prior, target)


def branch_kernel(share, count, normed_ref, w_ref, out_ref):
    owners, both, size = normed_ref.shape
    packed = both - count
    normed = normed_ref[:, :count, :].reshape(-1, size)
    weight = w_ref[1]
    total = jnp.dot(normed, weight, preferred_element_type=jnp.float32)
    at = lax.axis_index("tp") * share
    held = [normed_ref[:, count:, :].reshape(-1, size)]
    held.append(jnp.concatenate([normed_ref[n ^ 1, count:, :] for n in range(owners)], axis=0))
    groups = []
    for group in range(count // packed):
        kept = 0.0
        for half in range(2):
            place = selection(size, weight.shape[1], group * LANES + half * share, at, share)
            kept += jnp.dot(held[half], place, preferred_element_type=jnp.float32)
        groups.append(kept)
    rows = [groups[g][n * packed : (n + 1) * packed] for n in range(owners) for g in range(len(groups))]
    out_ref[...] = code(total + jnp.concatenate(rows, axis=0)).reshape(out_ref.shape)


def branch_parts(normed, weight, owners, count):
    return pl.pallas_call(
        functools.partial(branch_kernel, weight.shape[2] // owners, count),
        out_shape=jax.ShapeDtypeStruct((owners, normed.shape[0] * count // owners, weight.shape[2]), jnp.float32),
        compiler_params=PARAMS,
        name="branch",
    )(normed, weight)


def final_kernel(parts_ref, out_ref):
    out_ref[...] = decoded(parts_ref)


def layers(
    tokens,
    state,
    lengths,
    norm_gain,
    w_query,
    w_forget,
    w_input,
    w_gate,
    w_out,
    bound_logit,
    pace,
    head_gain,
):
    tp, dp = lax.axis_size("tp"), lax.axis_size("dp")
    whole = exchange(jnp.broadcast_to(tokens, (tp, *tokens.shape)), "tp")
    weights = (w_query, w_forget, w_input, w_gate)
    gain, *firsts = prep(norm_gain, weights)
    back = near(w_out[0], "dp")
    log_len = jnp.log(lengths.astype(jnp.float32) / LENGTH_MEAN)
    shift = pace[:, None, :] * log_len[None, :, None]

    message = project(whole, gain, firsts, dp).astype(jnp.float16)
    parts = exchange(message, "dp").astype(jnp.float32)
    target, own, sent = first(parts, shift, bound_logit, head_gain, tokens.shape[1] // tp, state)
    packed = pack(1, norm_gain, weights)
    held = near(packed, "dp")
    came = swap(sent, "dp")
    sums = pair_parts(own, came, back)
    parts = exchange_products(sums, "tp")
    copies = pl.pallas_call(
        next_kernel,
        out_shape=jax.ShapeDtypeStruct(parts.shape, jnp.bfloat16),
        compiler_params=PARAMS,
        name="next",
    )(parts)
    joined = exchange(after(copies, held[1:]), "tp")
    prior = load(after(gain, joined), state)
    own, sent, kept = again(joined, held, dp)
    came = swap(sent.astype(jnp.float16), "dp").astype(jnp.float32)
    target, normed = second(own, came, shift, bound_logit, head_gain, kept, prior, target)
    parts = exchange_products(branch_parts(exchange(normed, "dp"), w_out, tp, lengths.shape[0]), "tp")
    result = pl.pallas_call(
        final_kernel,
        out_shape=jax.ShapeDtypeStruct(tokens.shape, jnp.float32),
        compiler_params=PARAMS,
        name="final",
    )(parts)
    return result, target


def solution(mesh):
    in_specs = (
        P(("grp", "tp"), "dp"),
        P(None, ("grp", "dp"), "tp", None, None),
        P(("grp", "dp")),
        P(None, "dp"),
        P(None, "dp", "tp"),
        P(None, "dp", "tp"),
        P(None, "dp", "tp"),
        P(None, "dp", "tp"),
        P(None, "tp", "dp"),
        P(None, "tp"),
        P(None, "tp"),
        P(),
    )
    out_specs = (P(("grp", "tp"), "dp"), P(None, ("grp", "dp"), "tp", None, None))
    return jax.shard_map(layers, mesh=mesh, in_specs=in_specs, out_specs=out_specs, check_vma=False)
```
